512 devices in a mesh: sp: 16 (over z), fs: 4 (over y), tp: 8 (over x, core).
Axes of the slice: x: 4, y: 4, z: 16, core: 2. Of those that a mesh axis runs over, the one named last changes fastest.
Arguments:
- tokens: bfloat16 [4, 4096, 2048], P('fs', 'sp'), may hold values from -6 to 6
- norm_gain: float32 [2048], replicated, may hold values from 0.1 to 1.9
- w_state_in: bfloat16 [2048, 1024], P(('sp', 'fs'), 'tp'), may hold values from -0.125 to 0.125
- w_value: bfloat16 [2048, 1024], P(('sp', 'fs'), 'tp'), may hold values from -0.125 to 0.125
- w_outer: bfloat16 [2048, 1024], P(('sp', 'fs'), 'tp'), may hold values from -0.125 to 0.125
- w_inner: bfloat16 [2048, 1024], P(('sp', 'fs'), 'tp'), may hold values from -0.125 to 0.125
- w_state_out: bfloat16 [2048, 1024], P(('sp', 'fs'), 'tp'), may hold values from -0.125 to 0.125
- w_conv_out: bfloat16 [2048, 1024], P(('sp', 'fs'), 'tp'), may hold values from -0.125 to 0.125
- log_step: float32 [64], P('tp'), may hold values from -4.6 to -3.2
- decay_real: float32 [64, 64], P('tp'), may hold values from -5 to 0
- frequency: float32 [64, 64], P('tp'), may hold values from 1 to 192
- step_rate: float32 [4, 4096], P('fs', 'sp'), may hold values from 0.4 to 2.5
- input_real: float32 [64, 64, 16], P('tp'), may hold values from -1 to 1
- input_imag: float32 [64, 64, 16], P('tp'), may hold values from -1 to 1
- read_real: float32 [64, 16, 64], P('tp'), may hold values from -0.75 to 0.75
- read_imag: float32 [64, 16, 64], P('tp'), may hold values from -0.75 to 0.75
- skip_gain: float32 [64, 16], P('tp'), may hold values from -4 to 4
- conv_taps: float32 [3, 1024], P(None, 'tp'), may hold values from -3.5 to 3.5
- initial_state: float32 [4, 2, 64, 64], P('fs', None, 'tp'), may hold values from -6 to 6
Outputs:
- mixed: bfloat16 [4, 4096, 2048], P('fs', ('sp', 'tp'))
- final_state: float32 [4, 2, 64, 64], P('fs', None, 'tp', 'sp')
The draws below stay inside these ranges and needn't reach their ends.
All inputs are finite; a program needn't handle non-finite values.
Results may differ from the reference program's by a relative error of at most 0.018.
Values may be sent and summed in bfloat16 or wider, within the bound.
A program may use at most 64 MiB of HBM per device.

```python
import math
import jax
import jax.numpy as jnp
from jax import lax

D = 2048
GROUPS = 64
GROUP = 16
STATE = 64
CW = 1024
KW = 3
SW = 1024
SEQS = 4
LENGTH = 4096
N_TP = 8


def draw_decay_real(key, part):
    base = jax.random.fold_in(key, 7)
    key_pick, key_slow, key_fast = jax.random.split(base, 3)
    share = 0.5
    pick = jax.random.uniform(key_pick, (GROUPS, 1), jnp.float32) < share
    slow = -jnp.exp(jax.random.uniform(key_slow, (GROUPS, STATE), jnp.float32, math.log(5.0 / LENGTH), math.log(60.0 / LENGTH)))
    fast = -jnp.exp(jax.random.uniform(key_fast, (GROUPS, STATE), jnp.float32, math.log(2.0), math.log(5.0)))
    return jnp.where(pick, slow, fast)


def draw_step_rate(key, part):
    base = jax.random.fold_in(key, 13)
    key_slow, key_fine = jax.random.split(base, 2)
    blocks = LENGTH // 256
    slow = jnp.exp(jax.random.uniform(key_slow, (SEQS, blocks), jnp.float32, math.log(0.5), math.log(2.0)))
    fine = jax.random.uniform(key_fine, (SEQS, LENGTH), jnp.float32, 0.8, 1.25)
    return jnp.repeat(slow, 256, axis=1) * fine


def shard_levels(own_key, shape, cuts, smallest, top_value):
    level, own = 1.0, jax.random.fold_in(own_key, 6)
    for axis_at, parts in cuts:
        draws = jnp.exp(jax.random.uniform(jax.random.fold_in(own, axis_at), (parts,), jnp.float32, smallest / len(cuts), top_value / len(cuts)))
        level = level * jnp.repeat(draws, shape[axis_at] // parts).reshape([-1 if axis == axis_at else 1 for axis in range(len(shape))])
    return level


def noise(rng, shape, deviation, reach, pieces=(), kind=jnp.bfloat16):
    drawn = jax.random.normal(rng, shape, jnp.float32) * deviation
    if len(pieces) > 0:
        drawn = shard_levels(rng, shape, pieces, -0.22, 0.18) * drawn
    return jnp.clip(drawn, min=-reach, max=reach).astype(kind)


def setup_inputs(seed: int = 0) -> dict:
    streams_of = jax.random.split(jax.random.key(seed), 20)
    return {
        "tokens": noise(streams_of[0], (SEQS, LENGTH, D), 1.0, 6.0, ((0, 4), (1, 16))),
        "norm_gain": jnp.clip(1.0 + 0.18 * jax.random.normal(streams_of[1], (D,), jnp.float32), 0.1, 1.9),
        "w_state_in": noise(streams_of[2], (D, SW), D ** -0.5, 0.125, ((0, 64), (1, 8))),
        "w_value": noise(streams_of[3], (D, CW), D ** -0.5, 0.125, ((0, 64), (1, 8))),
        "w_outer": noise(streams_of[4], (D, CW), D ** -0.5, 0.125, ((0, 64), (1, 8))),
        "w_inner": noise(streams_of[5], (D, CW), D ** -0.5, 0.125, ((0, 64), (1, 8))),
        "w_state_out": noise(streams_of[6], (D, SW), (SW + CW) ** -0.5, 0.125, ((0, 64), (1, 8))),
        "w_conv_out": noise(streams_of[7], (D, CW), (SW + CW) ** -0.5, 0.125, ((0, 64), (1, 8))),
        "log_step": jnp.clip(-4.6 + 1.3999999 * jax.random.uniform(streams_of[8], (GROUPS,), jnp.float32) ** shard_levels(streams_of[8], (GROUPS,), ((0, 8),), -0.2, 0.2), -4.6, -3.2),
        "decay_real": draw_decay_real(jax.random.fold_in(streams_of[19], 71), 0),
        "frequency": jnp.clip(1.0 + 191.0 * jax.random.uniform(streams_of[10], (GROUPS, STATE), jnp.float32) ** shard_levels(streams_of[10], (GROUPS, STATE), ((0, 8),), -0.2, 0.2), 1.0, 192.0),
        "step_rate": draw_step_rate(jax.random.fold_in(streams_of[19], 71), 0),
        "input_real": noise(streams_of[12], (GROUPS, STATE, GROUP), (2 * GROUP) ** -0.5, 1.0, ((0, 8),), jnp.float32),
        "input_imag": noise(streams_of[13], (GROUPS, STATE, GROUP), (2 * GROUP) ** -0.5, 1.0, ((0, 8),), jnp.float32),
        "read_real": noise(streams_of[14], (GROUPS, GROUP, STATE), STATE ** -0.5, 0.75, ((0, 8),), jnp.float32),
        "read_imag": noise(streams_of[15], (GROUPS, GROUP, STATE), STATE ** -0.5, 0.75, ((0, 8),), jnp.float32),
        "skip_gain": noise(streams_of[16], (GROUPS, GROUP), 1.0, 4.0, ((0, 8),), jnp.float32),
        "conv_taps": noise(streams_of[17], (KW, CW), KW ** -0.5, 3.5, ((1, 8),), jnp.float32),
        "initial_state": noise(streams_of[18], (SEQS, 2, GROUPS, STATE), 1.0, 6.0, ((0, 4), (2, 8)), jnp.float32),
    }


def reference(tokens, norm_gain, w_state_in, w_value, w_outer, w_inner, w_state_out, w_conv_out, log_step, decay_real, frequency, step_rate, input_real, input_imag, read_real, read_imag, skip_gain, conv_taps, initial_state):
    seqs, length, width = tokens.shape
    features = tokens.astype(jnp.float32)
    mean_square = lax.optimization_barrier(jnp.mean(features * features, axis=-1, keepdims=True))
    normed = (features * lax.rsqrt(mean_square + 1e-06) * norm_gain).astype(jnp.bfloat16).reshape(seqs * length, width)

    def project(matrix):
        return jnp.dot(normed, matrix, preferred_element_type=jnp.float32).astype(jnp.bfloat16)
    state_in = project(w_state_in)
    value = project(w_value)
    outer = project(w_outer)
    inner = project(w_inner)
    groups, states = decay_real.shape
    group = skip_gain.shape[1]
    channels = state_in.astype(jnp.float32).reshape(seqs, length, groups, group)
    step = jnp.exp(log_step)[None, None, :] * step_rate[:, :, None]
    modulus = decay_real * decay_real + frequency * frequency

    def advance(carry, inputs):
        hidden_real, hidden_imag = carry
        chan_now, step_now = inputs
        scaled = step_now[..., None]
        grow = jnp.exp(scaled * decay_real)
        angle = scaled * frequency
        bar_real = grow * jnp.cos(angle)
        bar_imag = grow * jnp.sin(angle)
        less_real = bar_real - 1.0
        hold_real = (less_real * decay_real + bar_imag * frequency) / modulus
        hold_imag = (bar_imag * decay_real - less_real * frequency) / modulus
        drive_real = jnp.einsum('sgh,gph->sgp', chan_now, input_real, precision=lax.Precision.HIGHEST)
        drive_imag = jnp.einsum('sgh,gph->sgp', chan_now, input_imag, precision=lax.Precision.HIGHEST)
        push_real = hold_real * drive_real - hold_imag * drive_imag
        push_imag = hold_real * drive_imag + hold_imag * drive_real
        next_real = bar_real * hidden_real - bar_imag * hidden_imag + push_real
        next_imag = bar_real * hidden_imag + bar_imag * hidden_real + push_imag
        response = jnp.einsum('sgp,ghp->sgh', next_real, read_real, precision=lax.Precision.HIGHEST) - jnp.einsum('sgp,ghp->sgh', next_imag, read_imag, precision=lax.Precision.HIGHEST) + skip_gain * chan_now
        return ((next_real, next_imag), response)
    (last_real, last_imag), responses = lax.scan(advance, (initial_state[:, 0], initial_state[:, 1]), (channels.transpose(1, 0, 2, 3), step.transpose(1, 0, 2)))
    state_mix = jax.nn.gelu(responses.transpose(1, 0, 2, 3)).reshape(seqs * length, groups * group).astype(jnp.bfloat16)
    final_state = jnp.stack([last_real, last_imag], axis=1)
    gated = (inner.astype(jnp.float32) * value.astype(jnp.float32)).astype(jnp.bfloat16).reshape(seqs, length, -1)
    taps = conv_taps.shape[0]
    padded = jnp.pad(gated, ((0, 0), (taps - 1, 0), (0, 0))).astype(jnp.float32)
    filtered = jnp.zeros((seqs, length, gated.shape[2]), jnp.float32)
    for tap in range(taps):
        filtered = filtered + conv_taps[tap] * padded[:, tap:tap + length]
    conv_mix = (outer.astype(jnp.float32).reshape(seqs, length, -1) * filtered).astype(jnp.bfloat16).reshape(seqs * length, -1)
    state_block = state_mix.shape[1] // N_TP
    conv_block = conv_mix.shape[1] // N_TP
    total = jnp.zeros((seqs * length, width), jnp.float32)
    for block in range(N_TP):
        part = jnp.dot(state_mix[:, block * state_block:(block + 1) * state_block], w_state_out[:, block * state_block:(block + 1) * state_block].T, preferred_element_type=jnp.float32) + jnp.dot(conv_mix[:, block * conv_block:(block + 1) * conv_block], w_conv_out[:, block * conv_block:(block + 1) * conv_block].T, preferred_element_type=jnp.float32)
        total = total + lax.optimization_barrier(part.astype(jnp.bfloat16)).astype(jnp.float32)
    mixed = total.astype(jnp.bfloat16).reshape(seqs, length, width)
    return (mixed, final_state)
```

```python
import jax
import jax.numpy as jnp
from jax import lax
from jax.experimental import pallas as pl
from jax.experimental.pallas import tpu as pltpu
from jax.sharding import PartitionSpec as P


HIGHEST = lax.Precision.HIGHEST
MESH = pl.DeviceIdType.MESH
NZ, NY = 16, 4


def gather_kernel(*refs):
    shards = refs[:6]
    wg = refs[6]
    lsem, ya_s, ya_r, az_s, az_r, bz_s, bz_r, by_s, by_r = refs[7:]
    z = lax.axis_index("sp")
    y = lax.axis_index("fs")
    t = lax.axis_index("tp")
    zn, zp = lax.rem(z + 1, NZ), lax.rem(z + NZ - 1, NZ)

    barrier = pltpu.get_barrier_semaphore()
    for d in range(1, NY):
        pl.semaphore_signal(barrier, inc=1, device_id=(z, lax.rem(y + d, NY), t), device_id_type=MESH)
    for n in (zn, zp):
        pl.semaphore_signal(barrier, inc=1, device_id=(n, y, t), device_id_type=MESH)

    mine = pl.ds(pl.multiple_of(y * 32, 32), 32)
    local = [pltpu.make_async_copy(shards[w], wg.at[w, z, mine, :], lsem.at[w]) for w in range(6)]
    for c in local:
        c.start()
    pl.semaphore_wait(barrier, NY - 1 + 2)
    for c in local:
        c.wait()

    def a_y(d):
        return pltpu.make_async_remote_copy(
            wg.at[pl.ds(0, 3), z, mine, :], wg.at[pl.ds(0, 3), z, mine, :], ya_s.at[d - 1], ya_r.at[d - 1],
            device_id=(z, lax.rem(y + d, NY), t), device_id_type=MESH)

    def b_y(k, d):
        zb = lax.rem(z + k + NZ, NZ)
        return pltpu.make_async_remote_copy(
            wg.at[pl.ds(3, 3), zb, mine, :], wg.at[pl.ds(3, 3), zb, mine, :], by_s.at[zb, d - 1], by_r.at[zb, d - 1],
            device_id=(z, lax.rem(y + d, NY), t), device_id_type=MESH)

    def b_z(k, side):
        zb = lax.rem(z + (k if side else NZ - k), NZ)
        return pltpu.make_async_remote_copy(
            wg.at[pl.ds(3, 3), zb, mine, :], wg.at[pl.ds(3, 3), zb, mine, :], bz_s.at[side, k], bz_r.at[side, k],
            device_id=(zp if side else zn, y, t), device_id_type=MESH)

    def a_z(k, side, w):
        zb = lax.rem(z + (k if side else NZ - k), NZ)
        return pltpu.make_async_remote_copy(
            wg.at[w, zb], wg.at[w, zb], az_s.at[side, w, k], az_r.at[side, w, k],
            device_id=(zp if side else zn, y, t), device_id_type=MESH)

    for d in (2, 1, 3):
        a_y(d).start()
    for side in (0, 1):
        b_z(0, side).start()
    for d in (2, 1, 3):
        b_y(0, d).start()
    for d in (1, 3, 2):
        a_y(d).wait_recv()
    for w in range(3):
        for side in (0, 1):
            a_z(0, side, w).start()

    def step(k, right, left):
        sides = [s for s, on in ((0, right), (1, left)) if on is not None]
        fwd = {0: right, 1: left}
        for s in sides:
            b_z(k - 1, s).wait_recv()
            if fwd[s]:
                b_z(k, s).start()
            for d in (2, 1, 3):
                b_y(k if s else -k, d).start()
        for w in range(3):
            for s in sides:
                a_z(k - 1, s, w).wait_recv()
                if fwd[s]:
                    a_z(k, s, w).start()

    def loop(k, c):
        step(k, True, True)
        return c

    lax.fori_loop(1, 7, loop, 0)
    step(7, True, False)
    step(8, False, None)

    def drain_y(k, c):
        for d in (1, 2, 3):
            b_y(k, d).wait()
        return c

    lax.fori_loop(0, NZ, drain_y, 0)
    for d in (1, 2, 3):
        a_y(d).wait_send()

    def drain(k, c):
        for s in (0, 1):
            b_z(k, s).wait_send()
            for w in range(3):
                a_z(k, s, w).wait_send()
        return c

    lax.fori_loop(0, 7, drain, 0)
    b_z(7, 0).wait_send()
    for w in range(3):
        a_z(7, 0, w).wait_send()


def gather_weights(shards):
    return pl.pallas_call(
        gather_kernel,
        name="gather_weights",
        out_shape=jax.ShapeDtypeStruct((6, NZ, 128, 128), jnp.bfloat16),
        in_specs=[pl.BlockSpec(memory_space=pl.ANY)] * 6,
        out_specs=pl.BlockSpec(memory_space=pltpu.VMEM),
        scratch_shapes=[
            pltpu.SemaphoreType.DMA((6,)),
            pltpu.SemaphoreType.DMA((3,)),
            pltpu.SemaphoreType.DMA((3,)),
            pltpu.SemaphoreType.DMA((2, 3, 8)),
            pltpu.SemaphoreType.DMA((2, 3, 8)),
            pltpu.SemaphoreType.DMA((2, 8)),
            pltpu.SemaphoreType.DMA((2, 8)),
            pltpu.SemaphoreType.DMA((NZ, 3)),
            pltpu.SemaphoreType.DMA((NZ, 3)),
        ],
        compiler_params=pltpu.CompilerParams(collective_id=0, has_side_effects=True),
    )(*shards)


def in_one_piece(arrays, axis, dim, along):
    ends, at = ([], 0)
    for a in arrays[:-1]:
        at += a.shape[along]
        ends.append(at)
    both = jnp.concatenate(arrays, axis=along)
    return tuple(jnp.split(lax.all_gather(both, axis, axis=dim, tiled=True), ends, axis=along))


def laid_out(parts, dim):
    parts = jnp.moveaxis(parts, 0, dim)
    dims = parts.shape
    return parts.reshape(*dims[:dim], dims[dim] * dims[dim + 1], *dims[dim + 2 :])


def gather_together(arrays, axis, dims):
    ravelled = jnp.concatenate([a.reshape(-1) for a in arrays])
    lines, at, done = (lax.all_gather(ravelled, axis), 0, [])
    for a, dim in zip(arrays, dims):
        parts = lines[:, at : at + a.size].reshape(-1, *a.shape)
        done.append(laid_out(parts, dim))
        at += a.size
    return tuple(done)


def shifted(value, axis, steps):
    count = lax.axis_size(axis)
    initial, last = (max(0, -steps), min(count, count - steps))
    return lax.ppermute(value, axis, [(source, source + steps) for source in range(initial, last)])


def in_blocks(x, dim, length):
    before, after = (x.shape[:dim], x.shape[dim + 1 :])
    return jnp.moveaxis(x.reshape(*before, length, -1, *after), dim, 0)


def summed_on_arrival(x, axis, dim):
    length = lax.axis_size(axis)
    parts = lax.all_to_all(in_blocks(x, dim, length), axis, 0, 0, tiled=True)
    return jnp.sum(parts.astype(jnp.float32), axis=0)


def complex_product(left_real, left_imag, right_real, right_imag):
    return (
        left_real * right_real - left_imag * right_imag,
        left_real * right_imag + left_imag * right_real,
    )


def chain_pair(earlier, later):
    first_real, first_imag = complex_product(later[0], later[1], earlier[0], earlier[1])
    carry_real, carry_imag = complex_product(later[0], later[1], earlier[2], earlier[3])
    return (first_real, first_imag, carry_real + later[2], carry_imag + later[3])


def apply_map(summary, start_real, start_imag):
    moved_real, moved_imag = complex_product(summary[0], summary[1], start_real, start_imag)
    return (moved_real + summary[2], moved_imag + summary[3])


def body(
    tokens,
    norm_gain,
    w_state_in,
    w_value,
    w_outer,
    w_inner,
    w_state_out,
    w_conv_out,
    log_step,
    decay_real,
    frequency,
    step_rate,
    input_real,
    input_imag,
    read_real,
    read_imag,
    skip_gain,
    conv_taps,
    initial_state,
):
    rows = tokens.shape[1]
    features = tokens[0].astype(jnp.float32)
    mean_square = jnp.mean(features * features, axis=-1, keepdims=True)
    normed = (features * lax.rsqrt(mean_square + 1e-06) * norm_gain).astype(jnp.bfloat16)
    every_weight = gather_weights((w_state_in, w_value, w_state_out, w_inner, w_outer, w_conv_out))
    every_weight = every_weight.reshape(6, 2048, 128)
    weights = [every_weight[n] for n in (0, 1, 4, 3, 2, 5)]

    def project(matrix):
        return jnp.dot(normed, matrix, preferred_element_type=jnp.float32).astype(jnp.bfloat16)

    state_in = project(weights[0])
    value = project(weights[1])
    outer = project(weights[2])
    inner = project(weights[3])
    groups, states = decay_real.shape
    group = skip_gain.shape[1]
    flat = groups * states
    decay = decay_real.reshape(flat)
    turn_rate = frequency.reshape(flat)
    step = jnp.exp(log_step)[None, :] * step_rate[0][:, None]
    step_flat = jnp.repeat(step, states, axis=1)
    grow = jnp.exp(step_flat * decay)
    angle = step_flat * turn_rate
    bar_real = grow * jnp.cos(angle)
    bar_imag = grow * jnp.sin(angle)
    modulus = decay * decay + turn_rate * turn_rate
    less_real = bar_real - 1.0
    hold_real = (less_real * decay + bar_imag * turn_rate) / modulus
    hold_imag = (bar_imag * decay - less_real * turn_rate) / modulus
    channels = state_in.astype(jnp.float32).reshape(rows, groups, group)
    coupling = jnp.concatenate([input_real, input_imag], axis=1)
    driven = jnp.einsum("tgh,gqh->tgq", channels, coupling, precision=HIGHEST)
    drive_real = driven[:, :, :states].reshape(rows, flat)
    drive_imag = driven[:, :, states:].reshape(rows, flat)
    push_real, push_imag = complex_product(hold_real, hold_imag, drive_real, drive_imag)
    span = 16
    blocks = rows // span
    lower = (
        lax.broadcasted_iota(jnp.int32, (span, span), 0)
        >= lax.broadcasted_iota(jnp.int32, (span, span), 1)
    ).astype(jnp.float32)
    elapsed = jnp.einsum(
        "ts,bsf->btf", lower, step_flat.reshape(blocks, span, flat), precision=HIGHEST
    )
    rise = jnp.exp(decay * elapsed)
    phase = turn_rate * elapsed
    carry_real = rise * jnp.cos(phase)
    carry_imag = rise * jnp.sin(phase)
    fall = jnp.exp(-decay * elapsed)
    undo_real, undo_imag = complex_product(
        fall * jnp.cos(phase),
        -fall * jnp.sin(phase),
        push_real.reshape(blocks, span, flat),
        push_imag.reshape(blocks, span, flat),
    )
    summed = jnp.einsum(
        "ts,cbsf->cbtf", lower, jnp.stack([undo_real, undo_imag]), precision=HIGHEST
    )
    local_real, local_imag = complex_product(carry_real, carry_imag, summed[0], summed[1])
    ends = (carry_real[:, -1], carry_imag[:, -1], local_real[:, -1], local_imag[:, -1])
    inclusive = lax.associative_scan(chain_pair, ends, axis=0)
    unit_row = jnp.ones((1, flat), jnp.float32)
    empty_row = jnp.zeros((1, flat), jnp.float32)
    before = (
        jnp.concatenate([unit_row, inclusive[0][:-1]], axis=0),
        jnp.concatenate([empty_row, inclusive[1][:-1]], axis=0),
        jnp.concatenate([empty_row, inclusive[2][:-1]], axis=0),
        jnp.concatenate([empty_row, inclusive[3][:-1]], axis=0),
    )
    summary = (inclusive[0][-1], inclusive[1][-1], inclusive[2][-1], inclusive[3][-1])
    opening_state = initial_state[0].reshape(2, flat)
    every = gather_together(
        (summary[0][None], summary[1][None], summary[2][None], summary[3][None]), "sp", (0, 0, 0, 0)
    )
    running = lax.associative_scan(chain_pair, every, axis=0)
    position = lax.axis_index("sp")
    earlier = jnp.maximum(position - 1, 0)
    picked = [lax.dynamic_index_in_dim(piece, earlier, 0, keepdims=False) for piece in running]
    opening = position == 0
    prefix = (
        jnp.where(opening, 1.0, picked[0]),
        jnp.where(opening, 0.0, picked[1]),
        jnp.where(opening, 0.0, picked[2]),
        jnp.where(opening, 0.0, picked[3]),
    )
    enter_real, enter_imag = apply_map(prefix, opening_state[0], opening_state[1])
    total_map = (running[0][-1], running[1][-1], running[2][-1], running[3][-1])
    closing_real, closing_imag = apply_map(total_map, opening_state[0], opening_state[1])
    closing = jnp.stack([closing_real, closing_imag])
    block_real, block_imag = apply_map(before, enter_real[None], enter_imag[None])
    shift_real, shift_imag = complex_product(
        carry_real, carry_imag, block_real[:, None], block_imag[:, None]
    )
    hidden_real = (local_real + shift_real).reshape(rows, groups, states)
    hidden_imag = (local_imag + shift_imag).reshape(rows, groups, states)
    reading = jnp.concatenate([read_real, -read_imag], axis=2)
    joined = jnp.concatenate([hidden_real, hidden_imag], axis=2)
    response = jnp.einsum("tgq,ghq->tgh", joined, reading, precision=HIGHEST) + skip_gain * channels
    state_mix = jax.nn.gelu(response).reshape(rows, groups * group).astype(jnp.bfloat16)
    gated = (inner.astype(jnp.float32) * value.astype(jnp.float32)).astype(jnp.bfloat16)
    reach = conv_taps.shape[0] - 1
    earlier_rows = shifted(gated[rows - reach :], "sp", 1)
    extended = jnp.concatenate([earlier_rows, gated], axis=0).astype(jnp.float32)
    filtered = conv_taps[0] * extended[0:rows]
    for tap in range(1, reach + 1):
        filtered = filtered + conv_taps[tap] * extended[tap : tap + rows]
    conv_mix = (outer.astype(jnp.float32) * filtered).astype(jnp.bfloat16)
    mixed = summed_on_arrival(
        (
            jnp.einsum("rc,dc->rd", state_mix, weights[4], preferred_element_type=jnp.float32)
            + jnp.einsum("rc,dc->rd", conv_mix, weights[5], preferred_element_type=jnp.float32)
        ).astype(jnp.bfloat16),
        "tp",
        0,
    ).astype(jnp.bfloat16)
    share = states // lax.axis_size("sp")
    closing_grid = closing.reshape(2, groups, states)
    own_share = lax.dynamic_slice_in_dim(closing_grid, lax.axis_index("sp") * share, share, 2)
    return (mixed[None], own_share[None])


def solution(mesh):
    return jax.shard_map(
        body,
        mesh=mesh,
        in_specs=(
            P("fs", "sp", None),
            P(),
            P(("sp", "fs"), "tp"),
            P(("sp", "fs"), "tp"),
            P(("sp", "fs"), "tp"),
            P(("sp", "fs"), "tp"),
            P(("sp", "fs"), "tp"),
            P(("sp", "fs"), "tp"),
            P("tp"),
            P("tp", None),
            P("tp", None),
            P("fs", "sp"),
            P("tp", None, None),
            P("tp", None, None),
            P("tp", None, None),
            P("tp", None, None),
            P("tp", None),
            P(None, "tp"),
            P("fs", None, "tp", None),
        ),
        out_specs=(P("fs", ("sp", "tp"), None), P("fs", None, "tp", "sp")),
        check_vma=False,
    )
```

```python
import math

import jax
import jax.numpy as jnp
from jax import lax
from jax.experimental import pallas as pl
from jax.experimental.pallas import tpu as pltpu
from jax.sharding import PartitionSpec as P

MESH = pl.DeviceIdType.MESH
HIGHEST = lax.Precision.HIGHEST
F32, BF16 = jnp.float32, jnp.bfloat16
NZ, NY, NX = 16, 4, 4
ROWS, D, CH, FLAT = 256, 2048, 128, 512
NT = (((1,), (1,)), ((), ()))
NCHUNK = 4
CW = D // NCHUNK
SIN = [math.pi, -(math.pi**3) / 6, math.pi**5 / 120, -(math.pi**7) / 5040, math.pi**9 / 362880, -(math.pi**11) / 39916800]
COS = [1.0, -(math.pi**2) / 2, math.pi**4 / 24, -(math.pi**6) / 720, math.pi**8 / 40320, -(math.pi**10) / 3628800, math.pi**12 / 479001600]


def horner(coefs, x):
    total = jnp.full_like(x, coefs[-1])
    for c in coefs[-2::-1]:
        total = total * x + c
    return total


def complex_power(rate, turn, fall):
    u = rate * turn
    r = u - jnp.round(u)
    x = r * r
    s = r * horner(SIN, x)
    c = horner(COS, x)
    grow = jnp.exp2(rate * fall)
    return grow * (1.0 - 2.0 * (s * s)), grow * (2.0 * (s * c))


def iota(shape, dim):
    return lax.broadcasted_iota(jnp.int32, shape, dim)


def lanes4(x):
    return jnp.concatenate([x, x, x, x], axis=1)


def layer_kernel(*refs):
    n_small = 12
    tokens = refs[0]
    shards = refs[1:7]
    small = refs[7 : 7 + n_small]
    out, fin = refs[7 + n_small : 9 + n_small]
    rest = refs[9 + n_small :]
    small_v = rest[:n_small]
    (
        wg, tk, nb, prm, pk, ratep, tchunk, ring_t, br, bi, pc, dr, di, coup, readw, xp_s, ext, halo,
        ends, ec, hc, rows8, hd, mix, ps, pr, cs, rb,
        ssem, lsem, tsem, ya_s, ya_r, az_s, az_r, bz_s, bz_r, by_s, by_r, tz_s, tz_r, h_s, h_r, e_s, e_r,
        p_s, p_r, x_s, x_r,
    ) = rest[n_small:]
    gain, lstep, decay, freq, rate, in_r, in_i, rd_r, rd_i, skip, taps, init = small_v
    z = lax.axis_index("sp")
    y = lax.axis_index("fs")
    t = lax.axis_index("tp")
    xx, cc = t // 2, lax.rem(t, 2)
    other = 1 - cc
    zn, zp = lax.rem(z + 1, NZ), lax.rem(z + NZ - 1, NZ)

    loads = [pltpu.make_async_copy(s, v, ssem.at[n]) for n, (s, v) in enumerate(zip(small, small_v))]
    mine = pl.ds(pl.multiple_of(z * 128 + y * 32, 32), 32)
    local = [pltpu.make_async_copy(shards[w], wg.at[w, mine, :], lsem.at[w]) for w in range(6)]
    tok = pltpu.make_async_copy(tokens, tk, tsem)
    for c in local:
        c.start()
    for c in loads:
        c.start()
    tok.start()

    barrier = pltpu.get_barrier_semaphore()
    for d in range(1, NY):
        pl.semaphore_signal(barrier, inc=1, device_id=(z, lax.rem(y + d, NY), t), device_id_type=MESH)
    for n in (zn, zp):
        pl.semaphore_signal(barrier, inc=1, device_id=(n, y, t), device_id_type=MESH)
    for d in range(1, NX):
        pl.semaphore_signal(barrier, inc=1, device_id=(z, y, lax.rem(xx + d, NX) * 2 + cc), device_id_type=MESH)
    pl.semaphore_signal(barrier, inc=1, device_id=(z, y, xx * 2 + other), device_id_type=MESH)
    pl.semaphore_wait(barrier, 9)
    for c in local:
        c.wait()

    def a_y(d):
        return pltpu.make_async_remote_copy(
            wg.at[pl.ds(0, 3), mine, :], wg.at[pl.ds(0, 3), mine, :], ya_s.at[d - 1], ya_r.at[d - 1],
            device_id=(z, lax.rem(y + d, NY), t), device_id_type=MESH)

    def b_rows(zb):
        return pl.ds(pl.multiple_of(zb * 128 + y * 32, 32), 32)

    def b_y(k, d):
        zb = lax.rem(z + k + NZ, NZ)
        return pltpu.make_async_remote_copy(
            wg.at[pl.ds(3, 3), b_rows(zb), :], wg.at[pl.ds(3, 3), b_rows(zb), :], by_s.at[zb, d - 1], by_r.at[zb, d - 1],
            device_id=(z, lax.rem(y + d, NY), t), device_id_type=MESH)

    def b_z(k, side):
        zb = lax.rem(z + (k if side else NZ - k), NZ)
        return pltpu.make_async_remote_copy(
            wg.at[pl.ds(3, 3), b_rows(zb), :], wg.at[pl.ds(3, 3), b_rows(zb), :], bz_s.at[side, k], bz_r.at[side, k],
            device_id=(zp if side else zn, y, t), device_id_type=MESH)

    def a_z(k, side, w):
        zb = lax.rem(z + (k if side else NZ - k), NZ)
        rows = pl.ds(pl.multiple_of(zb * 128, 128), 128)
        return pltpu.make_async_remote_copy(
            wg.at[w, rows, :], wg.at[w, rows, :], az_s.at[side, w, k], az_r.at[side, w, k],
            device_id=(zp if side else zn, y, t), device_id_type=MESH)

    def t_z(k, side):
        zb = lax.rem(z + (k if side else NZ - k), NZ)
        return pltpu.make_async_remote_copy(
            ring_t.at[zb], ring_t.at[zb], tz_s.at[side, k], tz_r.at[side, k],
            device_id=(zp if side else zn, y, t), device_id_type=MESH)

    for d in (2, 1, 3):
        a_y(d).start()
    for side in (0, 1):
        b_z(0, side).start()
    for d in (2, 1, 3):
        b_y(0, d).start()

    for c in loads:
        c.wait()
    row, col = iota((ROWS, ROWS), 0), iota((ROWS, ROWS), 1)
    interleave = col == (row & 7) * 32 + (row >> 3)
    spread = jnp.where(interleave, rate[...], 0.0)
    ratep[...] = jnp.dot(spread, jnp.ones((ROWS, 128), F32), precision=HIGHEST, preferred_element_type=F32)
    totals = jnp.sum(ratep[...].reshape(32, 8, 128), axis=0)
    tchunk[...] = totals
    ring_t[z] = jnp.sum(totals, axis=0, keepdims=True)

    for d in (1, 3, 2):
        a_y(d).wait_recv()
    for w in range(3):
        for side in (0, 1):
            a_z(0, side, w).start()
    for side in (0, 1):
        t_z(0, side).start()

    tall = jnp.concatenate([decay[...], freq[...], init[...]], axis=0)
    hot = ((iota((64, FLAT), 1) & 63) == iota((64, FLAT), 0)).astype(F32)
    wide = jnp.dot(tall, hot, precision=HIGHEST, preferred_element_type=F32)
    own = (iota((8, FLAT), 1) >> 6) == iota((8, FLAT), 0)

    def line(v):
        return jnp.sum(jnp.where(own, v, 0.0), axis=0, keepdims=True)

    decay_l, freq_l = line(wide[0:8]), line(wide[8:16])
    dt = jnp.exp(line(jnp.broadcast_to(lstep[...], (8, FLAT))))
    modulus = decay_l * decay_l + freq_l * freq_l
    lines = [dt * freq_l * (0.5 / math.pi), dt * decay_l * math.log2(math.e), decay_l / modulus, -freq_l / modulus,
             line(wide[16:24]), line(wide[24:32])]
    for n, v in enumerate(lines):
        prm[n : n + 1, :] = v
        for i in range(4):
            pk[n, i : i + 1, :] = v[:, i * 128 : (i + 1) * 128]
    c_re, c_im = complex_power(lanes4(tchunk[...]), prm[0:1, :], prm[1:2, :])
    pc[0] = c_re
    pc[1] = c_im
    hot16 = ((iota((16, CH), 1) & 15) == iota((16, CH), 0)).astype(BF16)
    block = (iota((FLAT, CH), 0) >> 6) == (iota((FLAT, CH), 1) >> 4)
    for n, src in enumerate((in_r, in_i)):
        w = jnp.dot(src[...].astype(BF16), hot16, preferred_element_type=F32)
        coup[n * FLAT : (n + 1) * FLAT, :] = jnp.where(block, w, 0.0).astype(BF16)
    block_t = (iota((CH, FLAT), 1) >> 6) == (iota((CH, FLAT), 0) >> 4)
    hot64 = hot.astype(BF16)
    for n, src in enumerate((rd_r, rd_i)):
        w = jnp.dot(src[...].astype(BF16), hot64, preferred_element_type=F32)
        readw[:, n * FLAT : (n + 1) * FLAT] = jnp.where(block_t, w if n == 0 else -w, 0.0).astype(BF16)
    tok.wait()

    def work(k):
        rows = pl.ds(pl.multiple_of((k - 1) * 32, 32), 32)
        f = tk[rows, :].astype(F32)
        mean_square = jnp.mean(f * f, axis=-1, keepdims=True)
        nb[rows, :] = (f * lax.rsqrt(mean_square + 1e-06) * gain[...]).astype(BF16)
        for half in range(2):
            rows = pl.ds(pl.multiple_of((k - 1) * 32 + half * 16, 16), 16)
            re, im = complex_power(lanes4(ratep[rows, :]), prm[0:1, :], prm[1:2, :])
            br[rows, :] = re
            bi[rows, :] = im

    def step(k, right, left):
        sides = [s for s, on in ((0, right), (1, left)) if on is not None]
        fwd = {0: right, 1: left}
        for s in sides:
            b_z(k - 1, s).wait_recv()
            if fwd[s]:
                b_z(k, s).start()
            for d in (2, 1, 3):
                b_y(k if s else -k, d).start()
        for w in range(3):
            for s in sides:
                a_z(k - 1, s, w).wait_recv()
                if fwd[s]:
                    a_z(k, s, w).start()
        for s in sides:
            t_z(k - 1, s).wait_recv()
            if fwd[s]:
                t_z(k, s).start()
        work(k)

    def loop(k, c):
        step(k, True, True)
        return c

    lax.fori_loop(1, 7, loop, 0)
    step(7, True, False)
    step(8, False, None)

    def drain_y(k, c):
        for d in (1, 2, 3):
            b_y(k, d).wait_recv()
        return c

    def project(w):
        return jnp.dot(nb[...], wg[w], preferred_element_type=F32).astype(BF16)

    state_in = project(0)
    value = project(1).astype(F32)
    lax.fori_loop(0, NZ, drain_y, 0)
    inner = project(3).astype(F32)
    gated = (inner * value).astype(BF16).astype(F32)
    ext[8 : 8 + ROWS, :] = gated

    perm = jnp.where(interleave, 1.0, 0.0).astype(BF16)
    xp = jnp.dot(perm, state_in, preferred_element_type=F32)
    xp_s[...] = xp
    drive = lax.dot_general(xp.astype(BF16), coup[...], NT, preferred_element_type=F32)
    v_re, v_im = drive[:, :FLAT], drive[:, FLAT:]
    a_re, a_im = prm[2:3, :], prm[3:4, :]
    dr[...] = v_re * a_re - v_im * a_im
    di[...] = v_re * a_im + v_im * a_re
    h_copy = pltpu.make_async_remote_copy(
        ext.at[pl.ds(ROWS, 8), :], halo, h_s, h_r, device_id=(zn, y, t), device_id_type=MESH)
    h_copy.start()

    def advance(j, h):
        rows = pl.ds(pl.multiple_of(j * 8, 8), 8)
        b_re, b_im, d_re, d_im = br[rows, :], bi[rows, :], dr[rows, :], di[rows, :]
        re, im = h[0] + d_re, h[1] + d_im
        return (b_re * re - b_im * im - d_re, b_re * im + b_im * re - d_im)

    zero = jnp.zeros((8, FLAT), F32)
    end_re, end_im = lax.fori_loop(0, 32, advance, (zero, zero))
    ec[0] = end_re
    ec[1] = end_im

    def chain(re, im, keep):
        for c in range(8):
            if keep:
                hc[0, c : c + 1, :] = re
                hc[1, c : c + 1, :] = im
            p_re, p_im = pc[0, c : c + 1, :], pc[1, c : c + 1, :]
            re, im = (p_re * re - p_im * im + ec[0, c : c + 1, :], p_re * im + p_im * re + ec[1, c : c + 1, :])
        return re, im

    none = jnp.zeros((1, FLAT), F32)
    e_re, e_im = chain(none, none, False)
    for i in range(4):
        ends[z, i : i + 1, :] = e_re[:, i * 128 : (i + 1) * 128]
        ends[z, 4 + i : 5 + i, :] = e_im[:, i * 128 : (i + 1) * 128]

    outer = project(4).astype(F32)

    def e_copy(d):
        return pltpu.make_async_remote_copy(
            ends.at[z], ends.at[z], e_s.at[d - 1], e_r.at[d - 1],
            device_id=(lax.rem(z + d, NZ), y, t), device_id_type=MESH)

    for d in (8, 7, 9, 6, 10, 5, 11, 4, 12, 3, 13, 2, 14, 1, 15):
        e_copy(d).start()
    h_copy.wait_recv()
    ext[0:8, :] = jnp.where(z == 0, 0.0, halo[...])
    filtered = taps[0:1, :] * ext[6 : 6 + ROWS, :] + taps[1:2, :] * ext[7 : 7 + ROWS, :] + taps[2:3, :] * ext[8 : 8 + ROWS, :]
    mix[:, CH:] = (outer * filtered).astype(BF16)

    def span_power(j):
        return complex_power(ring_t[j], pk[0, 0:4, :], pk[1, 0:4, :])

    powers = [span_power(j) for j in range(NZ)]
    for d in range(1, NZ):
        e_copy(d).wait_recv()
    re, im = pk[4, 0:4, :], pk[5, 0:4, :]
    in_re, in_im = re, im
    for j in range(NZ):
        p_re, p_im = powers[j]
        re, im = (p_re * re - p_im * im + ends[j, 0:4, :], p_re * im + p_im * re + ends[j, 4:8, :])
        if j < NZ - 1:
            here = z == j + 1
            in_re, in_im = jnp.where(here, re, in_re), jnp.where(here, im, in_im)
    rows8[0, 0:4, :] = in_re
    rows8[0, 4:8, :] = in_im
    rows8[1, 0:4, :] = re
    rows8[1, 4:8, :] = im

    def as_line(n, at):
        return jnp.concatenate([rows8[n, at + i : at + i + 1, :] for i in range(4)], axis=1)

    chain(as_line(0, 0), as_line(0, 4), True)

    def advance2(i, h):
        one = advance(2 * i, h)
        two = advance(2 * i + 1, one)
        rows = pl.ds(pl.multiple_of(i * 16, 16), 16)
        hd[rows, :FLAT] = jnp.concatenate([one[0], two[0]], axis=0).astype(BF16)
        hd[rows, FLAT:] = jnp.concatenate([one[1], two[1]], axis=0).astype(BF16)
        return two

    lax.fori_loop(0, 16, advance2, (hc[0], hc[1]))
    skip_w = jnp.dot(skip[...], ((iota((16, CH), 1) & 15) == iota((16, CH), 0)).astype(F32), precision=HIGHEST, preferred_element_type=F32)
    skip_l = jnp.sum(jnp.where((iota((8, CH), 1) >> 4) == iota((8, CH), 0), skip_w, 0.0), axis=0, keepdims=True)
    v = lax.dot_general(hd[...], readw[...], NT, preferred_element_type=F32) + skip_l * xp_s[...]
    smix = (0.5 * v * (1.0 + jnp.tanh(0.7978845608028654 * (v + 0.044715 * (v * v * v))))).astype(BF16)
    back = jnp.where(col == (row & 31) * 8 + (row >> 5), 1.0, 0.0).astype(BF16)
    mix[:, :CH] = jnp.dot(back, smix, preferred_element_type=F32).astype(BF16)

    def rows_of(core):
        return jnp.concatenate([mix[pl.ds(pl.multiple_of(b * 64 + core * 32, 32), 32), :] for b in range(NX)], axis=0)

    def w_out(n):
        return jnp.concatenate([wg[2, n * CW : (n + 1) * CW, :], wg[5, n * CW : (n + 1) * CW, :]], axis=1)

    def p_copy(n):
        return pltpu.make_async_remote_copy(
            ps.at[n], pr.at[n], p_s.at[n], p_r.at[n], device_id=(z, y, xx * 2 + other), device_id_type=MESH)

    def x_copy(n, d):
        to = lax.rem(xx + d, NX)
        return pltpu.make_async_remote_copy(
            cs.at[n, to], rb.at[n, d - 1], x_s.at[n, d - 1], x_r.at[n, d - 1],
            device_id=(z, y, to * 2 + cc), device_id_type=MESH)

    theirs, ours = rows_of(other), rows_of(cc)
    for n in range(NCHUNK):
        ps[n] = lax.dot_general(theirs, w_out(n), NT, preferred_element_type=F32).astype(BF16)
        p_copy(n).start()
    for n in range(NCHUNK):
        part = lax.dot_general(ours, w_out(n), NT, preferred_element_type=F32)
        p_copy(n).wait_recv()
        cs[n] = (part + pr[n].astype(F32)).astype(BF16).reshape(NX, 32, CW)
        for d in (2, 1, 3):
            x_copy(n, d).start()
    far = jnp.where(own, jnp.broadcast_to(as_line(1, 0), (8, FLAT)), 0.0)
    far_i = jnp.where(own, jnp.broadcast_to(as_line(1, 4), (8, FLAT)), 0.0)
    pick = ((iota((FLAT, 4), 0) & 63) == z * 4 + iota((FLAT, 4), 1)).astype(F32)
    fin[0] = jnp.dot(far, pick, precision=HIGHEST, preferred_element_type=F32)
    fin[1] = jnp.dot(far_i, pick, precision=HIGHEST, preferred_element_type=F32)
    for n in range(NCHUNK):
        for d in (1, 3, 2):
            x_copy(n, d).wait_recv()
        total = cs[n, xx].astype(F32) + rb[n, 0].astype(F32) + rb[n, 1].astype(F32) + rb[n, 2].astype(F32)
        out[:, n * CW : (n + 1) * CW] = total.astype(BF16)

    for d in (1, 2, 3):
        a_y(d).wait_send()

    def drain_send(k, c):
        for d in (1, 2, 3):
            b_y(k, d).wait_send()
        return c

    lax.fori_loop(0, NZ, drain_send, 0)

    def drain(k, c):
        for s in (0, 1):
            b_z(k, s).wait_send()
            t_z(k, s).wait_send()
            for w in range(3):
                a_z(k, s, w).wait_send()
        return c

    lax.fori_loop(0, 7, drain, 0)
    b_z(7, 0).wait_send()
    t_z(7, 0).wait_send()
    for w in range(3):
        a_z(7, 0, w).wait_send()
    h_copy.wait_send()
    for d in range(1, NZ):
        e_copy(d).wait_send()
    for n in range(NCHUNK):
        p_copy(n).wait_send()
        for d in (1, 2, 3):
            x_copy(n, d).wait_send()


def body(
    tokens, norm_gain, w_state_in, w_value, w_outer, w_inner, w_state_out, w_conv_out, log_step, decay_real, frequency,
    step_rate, input_real, input_imag, read_real, read_imag, skip_gain, conv_taps, initial_state,
):
    small = (
        norm_gain.reshape(1, D), log_step.reshape(8, 1), decay_real, frequency, step_rate, input_real.reshape(FLAT, 16),
        input_imag.reshape(FLAT, 16), read_real.reshape(CH, 64), read_imag.reshape(CH, 64), skip_gain, conv_taps,
        initial_state.reshape(16, 64),
    )
    dma = pltpu.SemaphoreType.DMA
    anywhere = pl.BlockSpec(memory_space=pl.ANY)
    vmem = pl.BlockSpec(memory_space=pltpu.VMEM)
    mixed, final = pl.pallas_call(
        layer_kernel,
        name="layer",
        out_shape=(jax.ShapeDtypeStruct((32, D), BF16), jax.ShapeDtypeStruct((2, 8, 4), F32)),
        in_specs=[anywhere] * (7 + len(small)),
        out_specs=(vmem, vmem),
        scratch_shapes=[pltpu.VMEM(a.shape, a.dtype) for a in small]
        + [
            pltpu.VMEM((6, D, CH), BF16),
            pltpu.VMEM((ROWS, D), BF16),
            pltpu.VMEM((ROWS, D), BF16),
            pltpu.VMEM((8, FLAT), F32),
            pltpu.VMEM((6, 8, 128), F32),
            pltpu.VMEM((ROWS, 128), F32),
            pltpu.VMEM((8, 128), F32),
            pltpu.VMEM((NZ, 1, 128), F32),
            pltpu.VMEM((ROWS, FLAT), F32),
            pltpu.VMEM((ROWS, FLAT), F32),
            pltpu.VMEM((2, 8, FLAT), F32),
            pltpu.VMEM((ROWS, FLAT), F32),
            pltpu.VMEM((ROWS, FLAT), F32),
            pltpu.VMEM((2 * FLAT, CH), BF16),
            pltpu.VMEM((CH, 2 * FLAT), BF16),
            pltpu.VMEM((ROWS, CH), F32),
            pltpu.VMEM((8 + ROWS, CH), F32),
            pltpu.VMEM((8, CH), F32),
            pltpu.VMEM((NZ, 8, 128), F32),
            pltpu.VMEM((2, 8, FLAT), F32),
            pltpu.VMEM((2, 8, FLAT), F32),
            pltpu.VMEM((2, 8, 128), F32),
            pltpu.VMEM((ROWS, 2 * FLAT), BF16),
            pltpu.VMEM((ROWS, 2 * CH), BF16),
            pltpu.VMEM((NCHUNK, 128, CW), BF16),
            pltpu.VMEM((NCHUNK, 128, CW), BF16),
            pltpu.VMEM((NCHUNK, NX, 32, CW), BF16),
            pltpu.VMEM((NCHUNK, NX - 1, 32, CW), BF16),
            dma((len(small),)),
            dma((6,)),
            dma,
            dma((3,)), dma((3,)),
            dma((2, 3, 8)), dma((2, 3, 8)),
            dma((2, 8)), dma((2, 8)),
            dma((NZ, 3)), dma((NZ, 3)),
            dma((2, 8)), dma((2, 8)),
            dma, dma,
            dma((NZ - 1,)), dma((NZ - 1,)),
            dma((NCHUNK,)), dma((NCHUNK,)),
            dma((NCHUNK, 3)), dma((NCHUNK, 3)),
        ],
        compiler_params=pltpu.CompilerParams(collective_id=0, has_side_effects=True),
    )(tokens.reshape(ROWS, D), w_state_in, w_value, w_state_out, w_inner, w_outer, w_conv_out, *small)
    return (mixed.reshape(1, 32, D), final.reshape(1, 2, 8, 4))


def solution(mesh):
    return jax.shard_map(
        body,
        mesh=mesh,
        in_specs=(
            P("fs", "sp", None),
            P(),
            P(("sp", "fs"), "tp"),
            P(("sp", "fs"), "tp"),
            P(("sp", "fs"), "tp"),
            P(("sp", "fs"), "tp"),
            P(("sp", "fs"), "tp"),
            P(("sp", "fs"), "tp"),
            P("tp"),
            P("tp", None),
            P("tp", None),
            P("fs", "sp"),
            P("tp", None, None),
            P("tp", None, None),
            P("tp", None, None),
            P("tp", None, None),
            P("tp", None),
            P(None, "tp"),
            P("fs", None, "tp", None),
        ),
        out_specs=(P("fs", ("sp", "tp"), None), P("fs", None, "tp", "sp")),
        check_vma=False,
    )
```

```python
import math

import jax
import jax.numpy as jnp
from jax import lax
from jax.experimental import pallas as pl
from jax.experimental.pallas import tpu as pltpu
from jax.sharding import PartitionSpec as P

MESH = pl.DeviceIdType.MESH
HIGHEST = lax.Precision.HIGHEST
F32, BF16 = jnp.float32, jnp.bfloat16
NZ, NY, NX = 16, 4, 4
ROWS, D, CH, FLAT = 256, 2048, 128, 512
NT = (((1,), (1,)), ((), ()))
NCHUNK = 4
CW = D // NCHUNK
NEAR = 5
FAR_FIRST = (8, 7, 9, 6, 10, 5, 11, 4, 12, 3, 13, 2, 14, 1, 15)
SIN = [math.pi, -(math.pi**3) / 6, math.pi**5 / 120, -(math.pi**7) / 5040, math.pi**9 / 362880, -(math.pi**11) / 39916800]
COS = [1.0, -(math.pi**2) / 2, math.pi**4 / 24, -(math.pi**6) / 720, math.pi**8 / 40320, -(math.pi**10) / 3628800, math.pi**12 / 479001600]


def horner(coefs, x):
    total = jnp.full_like(x, coefs[-1])
    for c in coefs[-2::-1]:
        total = total * x + c
    return total


def complex_power(rate, turn, fall):
    u = rate * turn
    r = u - jnp.round(u)
    x = r * r
    s = r * horner(SIN, x)
    c = horner(COS, x)
    grow = jnp.exp2(rate * fall)
    return grow * (1.0 - 2.0 * (s * s)), grow * (2.0 * (s * c))


def iota(shape, dim):
    return lax.broadcasted_iota(jnp.int32, shape, dim)


def lanes4(x):
    return jnp.concatenate([x, x, x, x], axis=1)


def layer_kernel(*refs):
    n_small = 12
    tokens = refs[0]
    shards = refs[1:7]
    small = refs[7 : 7 + n_small]
    out, fin = refs[7 + n_small : 9 + n_small]
    rest = refs[9 + n_small :]
    small_v = rest[:n_small]
    (
        wb, tk, nb, prm, pk, ratep, tchunk, ring_t, br, bi, pc, dr, di, coup, readw, xp_s, ext, ht,
        ends, ec, hc, rows8, hd, mix, ps, pr, cs, rl, rb,
        ssem, lsem, tsem, bz_s, bz_r, by_s, by_r, br_r, bw_r, tz_s, tz_r, h_s, h_r, e_s, e_r,
        p_s, p_r, x_s, x_r,
    ) = rest[n_small:]
    gain, lstep, decay, freq, rate, in_r, in_i, rd_r, rd_i, skip, taps, init = small_v
    z = lax.axis_index("sp")
    y = lax.axis_index("fs")
    t = lax.axis_index("tp")
    xx, cc = t // 2, lax.rem(t, 2)
    other = 1 - cc
    zn = lax.rem(z + 1, NZ)

    barrier = pltpu.get_barrier_semaphore()
    for n in (z + 1, z + NZ - 1, z + 2, z + NZ - 2):
        pl.semaphore_signal(barrier, inc=1, device_id=(lax.rem(n, NZ), y, t), device_id_type=MESH)
    for d in range(1, NY):
        pl.semaphore_signal(barrier, inc=1, device_id=(z, lax.rem(y + d, NY), t), device_id_type=MESH)
    for d in (1, NX - 1):
        pl.semaphore_signal(barrier, inc=1, device_id=(z, y, lax.rem(xx + d, NX) * 2 + cc), device_id_type=MESH)
    pl.semaphore_signal(barrier, inc=1, device_id=(z, y, xx * 2 + other), device_id_type=MESH)

    loads = [pltpu.make_async_copy(s, v, ssem.at[n]) for n, (s, v) in enumerate(zip(small, small_v))]
    def take(ref, sem):
        pltpu.make_async_copy(ref, ref, sem).wait()

    local = [pltpu.make_async_copy(shards[w], wb.at[z, y, w], lsem) for w in range(6)]
    tok = pltpu.make_async_copy(tokens, tk, tsem)
    for c in local:
        c.start()
    for c in loads:
        c.start()
    tok.start()
    pl.semaphore_wait(barrier, 10)
    take(wb.at[0, 0], lsem)

    def at_distance(k, side):
        return lax.rem(z + (k if side else NZ - k), NZ)

    def of_part(rows, part):
        return rows.at[0] if part == 0 else rows.at[pl.ds(1, 3)] if part == 1 else rows.at[pl.ds(4, 2)]

    def b_z(part, k, side, hop):
        rows = of_part(wb.at[at_distance(k, side), y], part)
        return pltpu.make_async_remote_copy(
            rows, rows, bz_s, bz_r.at[part, side, k + hop - 1],
            device_id=(at_distance(hop, 1 - side), y, t), device_id_type=MESH)

    def w_y(k, side, d, came=0, further=False):
        zb = at_distance(k, side)
        rows = of_part(wb.at[zb, lax.rem(y - came + NY, NY)], 2)
        return pltpu.make_async_remote_copy(
            rows, rows, by_s, bw_r.at[zb] if further else by_r.at[3],
            device_id=(z, lax.rem(y + d, NY), t), device_id_type=MESH)

    def b_y(k, side, d, came=0, further=False):
        zb = at_distance(k, side)
        rows = wb.at[zb, lax.rem(y - came + NY, NY)]
        rows = rows.at[pl.ds(0, 4)] if k < NEAR else of_part(rows, 1)
        return pltpu.make_async_remote_copy(
            rows, rows, by_s, br_r.at[zb] if further else by_r.at[0 if k < NEAR else 2],
            device_id=(z, lax.rem(y + d, NY), t), device_id_type=MESH)

    def s_y(k, side, d):
        rows = wb.at[at_distance(k, side), y, 0]
        return pltpu.make_async_remote_copy(
            rows, rows, by_s, by_r.at[1], device_id=(z, lax.rem(y + d, NY), t), device_id_type=MESH)

    def t_copy(d):
        return pltpu.make_async_remote_copy(
            ring_t.at[z], ring_t.at[z], tz_s, tz_r, device_id=(lax.rem(z + d, NZ), y, t), device_id_type=MESH)

    for part in (0, 1, 2):
        for hop in (2, 1):
            for side in (0, 1):
                b_z(part, 0, side, hop).start()
    b_y(0, 0, 1, further=True).start()
    b_y(0, 0, 3).start()

    for c in loads:
        c.wait()
    row, col = iota((ROWS, ROWS), 0), iota((ROWS, ROWS), 1)
    interleave = col == (row & 7) * 32 + (row >> 3)
    spread = jnp.where(interleave, rate[...], 0.0)
    ratep[...] = jnp.dot(spread, jnp.ones((ROWS, 128), F32), precision=HIGHEST, preferred_element_type=F32)
    totals = jnp.sum(ratep[...].reshape(32, 8, 128), axis=0)
    tchunk[...] = totals
    ring_t[z] = jnp.sum(totals, axis=0, keepdims=True)

    h_copy = pltpu.make_async_remote_copy(
        tokens.at[pl.ds(ROWS - 8, 8), :], ht, h_s, h_r, device_id=(zn, y, t), device_id_type=MESH)
    h_copy.start()

    tall = jnp.concatenate([decay[...], freq[...], init[...]], axis=0)
    hot = ((iota((64, FLAT), 1) & 63) == iota((64, FLAT), 0)).astype(F32)
    wide = jnp.dot(tall, hot, precision=HIGHEST, preferred_element_type=F32)
    own = (iota((8, FLAT), 1) >> 6) == iota((8, FLAT), 0)

    def line(v):
        return jnp.sum(jnp.where(own, v, 0.0), axis=0, keepdims=True)

    decay_l, freq_l = line(wide[0:8]), line(wide[8:16])
    column = jnp.sum(jnp.where(iota((8, 8), 0) == iota((8, 8), 1), lstep[...], 0.0), axis=1, keepdims=True)
    dt = jnp.exp(line(jnp.broadcast_to(column, (8, FLAT))))
    modulus = decay_l * decay_l + freq_l * freq_l
    lines = [dt * freq_l * (0.5 / math.pi), dt * decay_l * math.log2(math.e), decay_l / modulus, -freq_l / modulus,
             line(wide[16:24]), line(wide[24:32])]
    for n, v in enumerate(lines):
        prm[n : n + 1, :] = v
        for i in range(4):
            pk[n, i : i + 1, :] = v[:, i * 128 : (i + 1) * 128]
    c_re, c_im = complex_power(lanes4(tchunk[...]), prm[0:1, :], prm[1:2, :])
    pc[0] = c_re
    pc[1] = c_im
    block_t = (iota((CH, FLAT), 1) >> 6) == (iota((CH, FLAT), 0) >> 4)
    hot64 = hot.astype(BF16)
    for n, (dst, src, sign) in enumerate(((coup, in_r, 1), (coup, in_i, 1), (readw, rd_r, 1), (readw, rd_i, -1))):
        w = jnp.dot(src[...].astype(BF16), hot64, preferred_element_type=F32)
        at = (n % 2) * FLAT
        dst[:, at : at + FLAT] = jnp.where(block_t, sign * w, 0.0).astype(BF16)
    tok.wait()

    def normalized(f):
        mean_square = jnp.mean(f * f, axis=-1, keepdims=True)
        return (f * lax.rsqrt(mean_square + 1e-06) * gain[...]).astype(BF16)

    def work(k):
        rows = pl.ds(pl.multiple_of((k - 1) * 32, 32), 32)
        nb[rows, :] = normalized(tk[rows, :].astype(F32))
        for half in range(2):
            rows = pl.ds(pl.multiple_of((k - 1) * 32 + half * 16, 16), 16)
            re, im = complex_power(lanes4(ratep[rows, :]), prm[0:1, :], prm[1:2, :])
            br[rows, :] = re
            bi[rows, :] = im

    def sides_of(k):
        return (0, 1) if 0 < k < 8 else (0,)

    def step_w(k):
        for s in sides_of(k):
            b_z(2, k - 1, s, 1).wait_recv()
            if k + 2 <= (7 if s else 8):
                b_z(2, k, s, 2).start()

    def send_w(k):
        for s in sides_of(k):
            for d in (1, 3):
                w_y(k, s, d, further=d == (3 if s else 1)).start()

    def relay_w(k):
        for s in (0, 1) if 0 < k < 8 else (0,):
            d = 3 if s else 1
            w_y(k, s, d, further=True).wait_recv()
            w_y(k, s, d, d).start()

    def step_b(k):
        sides = (0, 1) if k < 8 else (0,)
        for part in (0, 1):
            for s in sides:
                b_z(part, k - 1, s, 1).wait_recv()
                if k + 2 <= (7 if s else 8):
                    b_z(part, k, s, 2).start()
                if k >= NEAR and part == 0:
                    for d in (2, 1, 3):
                        s_y(k, s, d).start()
        for s in sides:
            for d in (1, 3):
                b_y(k, s, d, further=d == (3 if s else 1)).start()

    def relay(k):
        for s in (0, 1) if 0 < k < 8 else (0,):
            d = 3 if s else 1
            b_y(k, s, d, further=True).wait_recv()
            b_y(k, s, d, d).start()

    for stage in range(1, 5):
        with jax.named_scope(f"b{stage}"):
            step_b(2 * stage - 1)
            step_b(2 * stage)
        work(2 * stage - 1)
        work(2 * stage)
        with jax.named_scope(f"relay{stage}"):
            for k in ((), (0,), (1, 2), (3, 4))[stage - 1]:
                relay(k)
        with jax.named_scope(f"w{stage}"):
            for k in ((), (1, 2), (3, 4), (5, 6))[stage - 1]:
                step_w(k)
    for d in FAR_FIRST:
        t_copy(d).start()
    with jax.named_scope("relay58"):
        for k in (5, 6, 7, 8):
            relay(k)
    for k in range(7):
        send_w(k)
    h_copy.wait_recv()
    before = ht[...].astype(F32)
    nb[ROWS:, :] = normalized(jnp.concatenate([before, before], axis=0))
    take(wb.at[0:9, 0:2, 0:4], by_r.at[0])
    take(wb.at[0:7, 0:3, 0], by_r.at[1])

    def w_b(w, first=0, count=NZ):
        return wb[first : first + count, :, w].reshape(count * 128, CH)

    def project(w, rows=ROWS):
        return jnp.dot(nb[0:rows, :], w, preferred_element_type=F32).astype(BF16)

    state_in = project(w_b(0))
    perm = jnp.where(interleave, 1.0, 0.0).astype(BF16)
    xp = jnp.dot(perm, state_in, preferred_element_type=F32)
    xp_s[...] = xp
    drive = jnp.dot(xp.astype(BF16), coup[...], preferred_element_type=F32)
    v_re, v_im = drive[:, :FLAT], drive[:, FLAT:]
    a_re, a_im = prm[2:3, :], prm[3:4, :]
    dr[...] = v_re * a_re - v_im * a_im
    di[...] = v_re * a_im + v_im * a_re

    def advance(j, h):
        rows = pl.ds(pl.multiple_of(j * 8, 8), 8)
        b_re, b_im, d_re, d_im = br[rows, :], bi[rows, :], dr[rows, :], di[rows, :]
        re, im = h[0] + d_re, h[1] + d_im
        return (b_re * re - b_im * im - d_re, b_re * im + b_im * re - d_im)

    zero = jnp.zeros((8, FLAT), F32)
    end_re, end_im = lax.fori_loop(0, 32, advance, (zero, zero))
    ec[0] = end_re
    ec[1] = end_im

    def chain(re, im, keep):
        for c in range(8):
            if keep:
                hc[0, c : c + 1, :] = re
                hc[1, c : c + 1, :] = im
            p_re, p_im = pc[0, c : c + 1, :], pc[1, c : c + 1, :]
            re, im = (p_re * re - p_im * im + ec[0, c : c + 1, :], p_re * im + p_im * re + ec[1, c : c + 1, :])
        return re, im

    none = jnp.zeros((1, FLAT), F32)
    e_re, e_im = chain(none, none, False)
    for i in range(4):
        ends[z, i : i + 1, :] = e_re[:, i * 128 : (i + 1) * 128]
        ends[z, 4 + i : 5 + i, :] = e_im[:, i * 128 : (i + 1) * 128]

    def e_copy(d):
        return pltpu.make_async_remote_copy(
            ends.at[z], ends.at[z], e_s, e_r,
            device_id=(lax.rem(z + d, NZ), y, t), device_id_type=MESH)

    for d in FAR_FIRST:
        e_copy(d).start()

    for k in (7, 8):
        step_w(k)
        send_w(k)
    take(wb.at[0:7, 0:2, 0:3], by_r.at[2])
    value = project(w_b(1), ROWS + 16).astype(F32)
    inner = project(w_b(2), ROWS + 16).astype(F32)
    gated = (inner * value).astype(BF16).astype(F32)
    ext[8 : 8 + ROWS, :] = gated[:ROWS]
    ext[0:8, :] = jnp.where(z == 0, 0.0, gated[ROWS : ROWS + 8])
    with jax.named_scope("relay_w04"):
        for k in (0, 1, 2, 3, 4):
            relay_w(k)
    outer = project(w_b(3)).astype(F32)
    for k in (5, 6, 7, 8):
        relay_w(k)
    take(ring_t.at[0:15], tz_r)
    powers = [complex_power(ring_t[j], pk[0, 0:4, :], pk[1, 0:4, :]) for j in range(NZ)]
    filtered = taps[0:1, :] * ext[6 : 6 + ROWS, :] + taps[1:2, :] * ext[7 : 7 + ROWS, :] + taps[2:3, :] * ext[8 : 8 + ROWS, :]
    mix[:, CH:] = (outer * filtered).astype(BF16)

    take(ends.at[0:15], e_r)
    re, im = pk[4, 0:4, :], pk[5, 0:4, :]
    in_re, in_im = re, im
    for j in range(NZ):
        p_re, p_im = powers[j]
        re, im = (p_re * re - p_im * im + ends[j, 0:4, :], p_re * im + p_im * re + ends[j, 4:8, :])
        if j < NZ - 1:
            here = z == j + 1
            in_re, in_im = jnp.where(here, re, in_re), jnp.where(here, im, in_im)
    rows8[0, 0:4, :] = in_re
    rows8[0, 4:8, :] = in_im
    rows8[1, 0:4, :] = re
    rows8[1, 4:8, :] = im

    def as_line(n, at):
        return jnp.concatenate([rows8[n, at + i : at + i + 1, :] for i in range(4)], axis=1)

    chain(as_line(0, 0), as_line(0, 4), True)

    def advance2(i, h):
        one = advance(2 * i, h)
        two = advance(2 * i + 1, one)
        rows = pl.ds(pl.multiple_of(i * 16, 16), 16)
        hd[rows, :FLAT] = jnp.concatenate([one[0], two[0]], axis=0).astype(BF16)
        hd[rows, FLAT:] = jnp.concatenate([one[1], two[1]], axis=0).astype(BF16)
        return two

    lax.fori_loop(0, 16, advance2, (hc[0], hc[1]))
    skip_w = jnp.dot(skip[...], ((iota((16, CH), 1) & 15) == iota((16, CH), 0)).astype(F32), precision=HIGHEST, preferred_element_type=F32)
    skip_l = jnp.sum(jnp.where((iota((8, CH), 1) >> 4) == iota((8, CH), 0), skip_w, 0.0), axis=0, keepdims=True)
    v = lax.dot_general(hd[...], readw[...], NT, preferred_element_type=F32) + skip_l * xp_s[...]
    smix = (0.5 * v * (1.0 + jnp.tanh(0.7978845608028654 * (v + 0.044715 * (v * v * v))))).astype(BF16)
    back = jnp.where(col == (row & 31) * 8 + (row >> 5), 1.0, 0.0).astype(BF16)
    mix[:, :CH] = jnp.dot(back, smix, preferred_element_type=F32).astype(BF16)

    def rows_of(core):
        return jnp.concatenate([mix[pl.ds(pl.multiple_of(b * 64 + core * 32, 32), 32), :] for b in range(NX)], axis=0)

    def w_out(n):
        return jnp.concatenate([w_b(4, n * NZ // NCHUNK, NZ // NCHUNK), w_b(5, n * NZ // NCHUNK, NZ // NCHUNK)], axis=1)

    def p_copy(n):
        return pltpu.make_async_remote_copy(
            ps.at[n], pr.at[n], p_s, p_r.at[n], device_id=(z, y, xx * 2 + other), device_id_type=MESH)

    def x_copy(n, kind):
        up = 1 if n % 2 == 0 else NX - 1
        d = up if kind < 2 else NX - up
        src = (cs.at[n, lax.rem(xx + 2, NX)], rl.at[n, 1], cs.at[n, lax.rem(xx + NX - up, NX)])[kind]
        dst = (rl.at[n, 0], rb.at[n, 0], rb.at[n, 1])[kind]
        return pltpu.make_async_remote_copy(
            src, dst, x_s, x_r.at[min(kind, 1), n],
            device_id=(z, y, lax.rem(xx + d, NX) * 2 + cc), device_id_type=MESH)

    take(wb.at[:, :, 0], by_r.at[3])
    theirs, ours = rows_of(other), rows_of(cc)
    for n in range(NCHUNK):
        ps[n] = lax.dot_general(theirs, w_out(n), NT, preferred_element_type=F32).astype(BF16)
        p_copy(n).start()
    for n in range(NCHUNK):
        part = lax.dot_general(ours, w_out(n), NT, preferred_element_type=F32)
        p_copy(n).wait_recv()
        cs[n] = (part + pr[n].astype(F32)).astype(BF16).reshape(NX, 32, CW)
        x_copy(n, 0).start()
    for n in range(NCHUNK):
        x_copy(n, 2).start()
    far = jnp.where(own, jnp.broadcast_to(as_line(1, 0), (8, FLAT)), 0.0)
    far_i = jnp.where(own, jnp.broadcast_to(as_line(1, 4), (8, FLAT)), 0.0)
    pick = ((iota((4, FLAT), 1) & 63) == z * 4 + iota((4, FLAT), 0)).astype(F32)
    fin[0] = lax.dot_general(pick, far, NT, precision=HIGHEST, preferred_element_type=F32)
    fin[1] = lax.dot_general(pick, far_i, NT, precision=HIGHEST, preferred_element_type=F32)
    for n in range(NCHUNK):
        to = lax.rem(xx + (1 if n % 2 == 0 else NX - 1), NX)
        x_copy(n, 0).wait_recv()
        rl[n, 1] = (rl[n, 0].astype(F32) + cs[n, to].astype(F32)).astype(BF16)
        x_copy(n, 1).start()
    for n in range(NCHUNK):
        take(rb.at[n], x_r.at[1, n])
        total = cs[n, xx].astype(F32) + rb[n, 0].astype(F32) + rb[n, 1].astype(F32)
        out[:, n * CW : (n + 1) * CW] = total.astype(BF16)

    take(wb.at[0:12], by_s)
    take(wb.at[0:15, 0], bz_s)
    h_copy.wait_send()
    take(ring_t.at[0:15], tz_s)
    take(ends.at[0:15], e_s)
    take(ps, p_s)
    take(cs.at[0:3], x_s)


def body(
    tokens, norm_gain, w_state_in, w_value, w_outer, w_inner, w_state_out, w_conv_out, log_step, decay_real, frequency,
    step_rate, input_real, input_imag, read_real, read_imag, skip_gain, conv_taps, initial_state,
):
    small = (
        norm_gain.reshape(1, D), log_step.reshape(1, 8), decay_real, frequency, step_rate,
        input_real.transpose(0, 2, 1).reshape(CH, 64), input_imag.transpose(0, 2, 1).reshape(CH, 64), read_real.reshape(CH, 64), read_imag.reshape(CH, 64), skip_gain, conv_taps,
        initial_state.reshape(16, 64),
    )
    dma = pltpu.SemaphoreType.DMA
    anywhere = pl.BlockSpec(memory_space=pl.ANY)
    vmem = pl.BlockSpec(memory_space=pltpu.VMEM)
    mixed, final = pl.pallas_call(
        layer_kernel,
        name="layer",
        out_shape=(pltpu.VMEM((32, D), BF16), pltpu.VMEM((2, 4, 8), F32)),
        in_specs=[anywhere] * (7 + len(small)),
        out_specs=(vmem, vmem),
        scratch_shapes=[pltpu.VMEM(a.shape, a.dtype) for a in small]
        + [
            pltpu.VMEM((NZ, NY, 6, 32, CH), BF16),
            pltpu.VMEM((ROWS, D), BF16),
            pltpu.VMEM((ROWS + 16, D), BF16),
            pltpu.VMEM((8, FLAT), F32),
            pltpu.VMEM((6, 8, 128), F32),
            pltpu.VMEM((ROWS, 128), F32),
            pltpu.VMEM((8, 128), F32),
            pltpu.VMEM((NZ, 1, 128), F32),
            pltpu.VMEM((ROWS, FLAT), F32),
            pltpu.VMEM((ROWS, FLAT), F32),
            pltpu.VMEM((2, 8, FLAT), F32),
            pltpu.VMEM((ROWS, FLAT), F32),
            pltpu.VMEM((ROWS, FLAT), F32),
            pltpu.VMEM((CH, 2 * FLAT), BF16),
            pltpu.VMEM((CH, 2 * FLAT), BF16),
            pltpu.VMEM((ROWS, CH), F32),
            pltpu.VMEM((8 + ROWS, CH), F32),
            pltpu.VMEM((8, D), BF16),
            pltpu.VMEM((NZ, 8, 128), F32),
            pltpu.VMEM((2, 8, FLAT), F32),
            pltpu.VMEM((2, 8, FLAT), F32),
            pltpu.VMEM((2, 8, 128), F32),
            pltpu.VMEM((ROWS, 2 * FLAT), BF16),
            pltpu.VMEM((ROWS, 2 * CH), BF16),
            pltpu.VMEM((NCHUNK, 128, CW), BF16),
            pltpu.VMEM((NCHUNK, 128, CW), BF16),
            pltpu.VMEM((NCHUNK, NX, 32, CW), BF16),
            pltpu.VMEM((NCHUNK, 2, 32, CW), BF16),
            pltpu.VMEM((NCHUNK, 2, 32, CW), BF16),
            dma((len(small),)),
            dma,
            dma,
            dma, dma((3, 2, 8)),
            dma, dma((4,)), dma((NZ,)), dma((NZ,)),
            dma, dma,
            dma, dma,
            dma, dma,
            dma, dma((NCHUNK,)),
            dma, dma((2, NCHUNK)),
        ],
        compiler_params=pltpu.CompilerParams(collective_id=0, has_side_effects=True),
    )(tokens.reshape(ROWS, D), w_state_in, w_value, w_inner, w_outer, w_state_out, w_conv_out, *small)
    return (mixed.reshape(1, 32, D), final.transpose(0, 2, 1).reshape(1, 2, 8, 4))


def solution(mesh):
    return jax.shard_map(
        body,
        mesh=mesh,
        in_specs=(
            P("fs", "sp", None),
            P(),
            P(("sp", "fs"), "tp"),
            P(("sp", "fs"), "tp"),
            P(("sp", "fs"), "tp"),
            P(("sp", "fs"), "tp"),
            P(("sp", "fs"), "tp"),
            P(("sp", "fs"), "tp"),
            P("tp"),
            P("tp", None),
            P("tp", None),
            P("fs", "sp"),
            P("tp", None, None),
            P("tp", None, None),
            P("tp", None, None),
            P("tp", None, None),
            P("tp", None),
            P(None, "tp"),
            P("fs", None, "tp", None),
        ),
        out_specs=(P("fs", ("sp", "tp"), None), P("fs", None, "tp", "sp")),
        check_vma=False,
    )
```

```python
import math

import jax
import jax.numpy as jnp
from jax import lax
from jax.experimental import pallas as pl
from jax.experimental.pallas import tpu as pltpu
from jax.sharding import PartitionSpec as P

MESH = pl.DeviceIdType.MESH
HIGHEST = lax.Precision.HIGHEST
F32, BF16 = jnp.float32, jnp.bfloat16
NZ, NY, NX = 16, 4, 4
ROWS, D, CH, FLAT = 256, 2048, 128, 512
NT = (((1,), (1,)), ((), ()))
NCHUNK = 4
CW = D // NCHUNK
NEAR = 3
FAR_FIRST = (8, 7, 9, 6, 10, 5, 11, 4, 12, 3, 13, 2, 14, 1, 15)
SIN = [math.pi, -(math.pi**3) / 6, math.pi**5 / 120, -(math.pi**7) / 5040, math.pi**9 / 362880, -(math.pi**11) / 39916800]
COS = [1.0, -(math.pi**2) / 2, math.pi**4 / 24, -(math.pi**6) / 720, math.pi**8 / 40320, -(math.pi**10) / 3628800, math.pi**12 / 479001600]


def horner(coefs, x):
    total = jnp.full_like(x, coefs[-1])
    for c in coefs[-2::-1]:
        total = total * x + c
    return total


def complex_power(rate, turn, fall):
    u = rate * turn
    r = u - jnp.round(u)
    x = r * r
    s = r * horner(SIN, x)
    c = horner(COS, x)
    grow = jnp.exp2(rate * fall)
    return grow * (1.0 - 2.0 * (s * s)), grow * (2.0 * (s * c))


def iota(shape, dim):
    return lax.broadcasted_iota(jnp.int32, shape, dim)


def lanes4(x):
    return jnp.concatenate([x, x, x, x], axis=1)


def layer_kernel(*refs):
    n_small = 12
    tokens = refs[0]
    shards = refs[1:7]
    small = refs[7 : 7 + n_small]
    out, fin = refs[7 + n_small : 9 + n_small]
    rest = refs[9 + n_small :]
    small_v = rest[:n_small]
    (
        wa, wb, tk, nb, nbp, prm, pk, ratep, tchunk, ring_t, br, bi, pc, dr, di, coup, readw, xp_s, ext, ht,
        ends, ec, hc, rows8, hd, way_back, mix, ps, pr, cs, rl, rb,
        ssem, lsem, tsem, ya_s, ya_r, az_s, az_r, bz_s, bz_r, by_s, by_r, br_r, bw_r, tz_s, tz_r, h_s, h_r, e_s, e_r,
        p_s, p_r, x_s, x_r,
    ) = rest[n_small:]
    gain, lstep, decay, freq, rate, in_r, in_i, rd_r, rd_i, skip, taps, init = small_v
    z = lax.axis_index("sp")
    y = lax.axis_index("fs")
    t = lax.axis_index("tp")
    xx, cc = t // 2, lax.rem(t, 2)
    other = 1 - cc
    zn = lax.rem(z + 1, NZ)

    barrier = pltpu.get_barrier_semaphore()
    for n in (z + 1, z + NZ - 1, z + 2, z + NZ - 2):
        pl.semaphore_signal(barrier, inc=1, device_id=(lax.rem(n, NZ), y, t), device_id_type=MESH)
    for d in range(1, NY):
        pl.semaphore_signal(barrier, inc=1, device_id=(z, lax.rem(y + d, NY), t), device_id_type=MESH)
    for d in (1, NX - 1):
        pl.semaphore_signal(barrier, inc=1, device_id=(z, y, lax.rem(xx + d, NX) * 2 + cc), device_id_type=MESH)
    pl.semaphore_signal(barrier, inc=1, device_id=(z, y, xx * 2 + other), device_id_type=MESH)

    loads = [pltpu.make_async_copy(s, v, ssem.at[n]) for n, (s, v) in enumerate(zip(small, small_v))]
    def take(ref, sem):
        pltpu.make_async_copy(ref, ref, sem).wait()

    local = [pltpu.make_async_copy(shards[w], wb.at[z, y, w], lsem) for w in range(5)]
    mine = pl.ds(pl.multiple_of(z * 128 + y * 32, 32), 32)
    local.append(pltpu.make_async_copy(shards[5], wa.at[mine, :], lsem))
    tok = pltpu.make_async_copy(tokens, tk, tsem)
    for c in local:
        c.start()
    for c in loads:
        c.start()
    tok.start()
    pl.semaphore_wait(barrier, 10)
    take(wb.at[0, 0:2, 0:3], lsem)

    def sides_of(k):
        return (0, 1) if 0 < k < 8 else (0,)

    def at_distance(k, side):
        return lax.rem(z + (k if side else NZ - k), NZ)

    def a_y(d):
        return pltpu.make_async_remote_copy(
            wa.at[mine, :], wa.at[mine, :], ya_s, ya_r, device_id=(z, lax.rem(y + d, NY), t), device_id_type=MESH)

    def a_z(k, side, part=None):
        at = at_distance(k, side) * 128
        rows = pl.ds(pl.multiple_of(at, 128), 128)
        if part is not None:
            rows = pl.ds(pl.multiple_of(at + part * 64, 64), 64)
        return pltpu.make_async_remote_copy(
            wa.at[rows, :], wa.at[rows, :], az_s, az_r.at[side, k],
            device_id=(at_distance(1, 1 - side), y, t), device_id_type=MESH)

    def step_a(k, last=False):
        for s in (0, 1):
            a_z(k - 1, s).wait_recv()
            a_z(k, s, s if last else None).start()

    def of_part(rows, part):
        return rows.at[0] if part == 0 else rows.at[pl.ds(1, 3)] if part == 1 else rows.at[pl.ds(4, 1)]

    def b_z(part, k, side, hop):
        rows = of_part(wb.at[at_distance(k, side), y], part)
        return pltpu.make_async_remote_copy(
            rows, rows, bz_s, bz_r.at[part, side, k + hop - 1],
            device_id=(at_distance(hop, 1 - side), y, t), device_id_type=MESH)

    def w_y(k, side, d, came=0, further=False):
        zb = at_distance(k, side)
        rows = of_part(wb.at[zb, lax.rem(y - came + NY, NY)], 2)
        return pltpu.make_async_remote_copy(
            rows, rows, by_s, bw_r.at[zb] if further else by_r.at[3],
            device_id=(z, lax.rem(y + d, NY), t), device_id_type=MESH)

    def b_y(k, side, d, came=0, further=False):
        zb = at_distance(k, side)
        rows = wb.at[zb, lax.rem(y - came + NY, NY)]
        rows = rows.at[pl.ds(0, 4)] if k < NEAR else of_part(rows, 1)
        return pltpu.make_async_remote_copy(
            rows, rows, by_s, br_r.at[zb] if further else by_r.at[0 if k < NEAR else 2],
            device_id=(z, lax.rem(y + d, NY), t), device_id_type=MESH)

    def s_y(k, side, d):
        rows = wb.at[at_distance(k, side), y, 0]
        return pltpu.make_async_remote_copy(
            rows, rows, by_s, by_r.at[1], device_id=(z, lax.rem(y + d, NY), t), device_id_type=MESH)

    def t_copy(d):
        return pltpu.make_async_remote_copy(
            ring_t.at[z], ring_t.at[z], tz_s, tz_r, device_id=(lax.rem(z + d, NZ), y, t), device_id_type=MESH)

    for part in (0, 1, 2):
        for hop in (2, 1):
            for side in (0, 1):
                b_z(part, 0, side, hop).start()
    for d in (2, 1, 3):
        a_y(d).start()
    b_y(0, 0, 1, further=True).start()
    b_y(0, 0, 3).start()

    for c in loads:
        c.wait()
    row, col = iota((ROWS, ROWS), 0), iota((ROWS, ROWS), 1)
    interleave = col == (row & 7) * 32 + (row >> 3)
    spread = jnp.where(interleave, rate[...], 0.0)
    ratep[...] = jnp.dot(spread, jnp.ones((ROWS, 128), F32), precision=HIGHEST, preferred_element_type=F32)
    totals = jnp.sum(ratep[...].reshape(32, 8, 128), axis=0)
    tchunk[...] = totals
    ring_t[z] = jnp.sum(totals, axis=0, keepdims=True)

    take(wb.at[0, 0, 0:3], ya_r)
    for side in (0, 1):
        a_z(0, side).start()
    h_copy = pltpu.make_async_remote_copy(
        tokens.at[pl.ds(ROWS - 8, 8), :], ht, h_s, h_r, device_id=(zn, y, t), device_id_type=MESH)
    h_copy.start()

    tall = jnp.concatenate([decay[...], freq[...], init[...]], axis=0)
    hot = ((iota((64, FLAT), 1) & 63) == iota((64, FLAT), 0)).astype(F32)
    wide = jnp.dot(tall, hot, precision=HIGHEST, preferred_element_type=F32)
    own = (iota((8, FLAT), 1) >> 6) == iota((8, FLAT), 0)

    def line(v):
        return jnp.sum(jnp.where(own, v, 0.0), axis=0, keepdims=True)

    decay_l, freq_l = line(wide[0:8]), line(wide[8:16])
    column = jnp.sum(jnp.where(iota((8, 8), 0) == iota((8, 8), 1), lstep[...], 0.0), axis=1, keepdims=True)
    dt = jnp.exp(line(jnp.broadcast_to(column, (8, FLAT))))
    modulus = decay_l * decay_l + freq_l * freq_l
    lines = [dt * freq_l * (0.5 / math.pi), dt * decay_l * math.log2(math.e), decay_l / modulus, -freq_l / modulus,
             line(wide[16:24]), line(wide[24:32])]
    for n, v in enumerate(lines):
        prm[n : n + 1, :] = v
        for i in range(4):
            pk[n, i : i + 1, :] = v[:, i * 128 : (i + 1) * 128]
    c_re, c_im = complex_power(lanes4(tchunk[...]), prm[0:1, :], prm[1:2, :])
    pc[0] = c_re
    pc[1] = c_im
    block_t = (iota((CH, FLAT), 1) >> 6) == (iota((CH, FLAT), 0) >> 4)
    hot64 = hot.astype(BF16)
    for n, (dst, src, sign) in enumerate(((coup, in_r, 1), (coup, in_i, 1), (readw, rd_r, 1), (readw, rd_i, -1))):
        w = jnp.dot(src[...].astype(BF16), hot64, preferred_element_type=F32)
        at = (n % 2) * FLAT
        dst[:, at : at + FLAT] = jnp.where(block_t, sign * w, 0.0).astype(BF16)
    tok.wait()

    def normalized(f):
        mean_square = jnp.mean(f * f, axis=-1, keepdims=True)
        return (f * lax.rsqrt(mean_square + 1e-06) * gain[...]).astype(BF16)

    def work(k):
        rows = pl.ds(pl.multiple_of((k - 1) * 32, 32), 32)
        nb[rows, :] = normalized(tk[rows, :].astype(F32))
        for half in range(2):
            rows = pl.ds(pl.multiple_of((k - 1) * 32 + half * 16, 16), 16)
            re, im = complex_power(lanes4(ratep[rows, :]), prm[0:1, :], prm[1:2, :])
            br[rows, :] = re
            bi[rows, :] = im

    def step_w(k):
        for s in sides_of(k):
            b_z(2, k - 1, s, 1).wait_recv()
            if k + 2 <= (7 if s else 8):
                b_z(2, k, s, 2).start()

    def send_w(k):
        for s in sides_of(k):
            for d in (1, 3):
                w_y(k, s, d, further=d == (3 if s else 1)).start()

    def relay_w(k):
        for s in (0, 1) if 0 < k < 8 else (0,):
            d = 3 if s else 1
            w_y(k, s, d, further=True).wait_recv()
            w_y(k, s, d, d).start()

    def step_b(pair, between):
        for part in (0, 1):
            for k in pair:
                for s in sides_of(k):
                    b_z(part, k - 1, s, 1).wait_recv()
                    if k + 2 <= (7 if s else 8):
                        b_z(part, k, s, 2).start()
                    if k >= NEAR and part == 0:
                        for d in (2, 1, 3):
                            s_y(k, s, d).start()
            if part == 0 and between:
                step_a(between)
        for k in pair:
            for s in sides_of(k):
                for d in (1, 3):
                    b_y(k, s, d, further=d == (3 if s else 1)).start()

    def relay(k):
        for s in (0, 1) if 0 < k < 8 else (0,):
            d = 3 if s else 1
            b_y(k, s, d, further=True).wait_recv()
            b_y(k, s, d, d).start()

    for stage in range(1, 5):
        with jax.named_scope(f"b{stage}"):
            step_b((2 * stage - 1, 2 * stage), stage if stage > 1 else None)
        work(2 * stage - 1)
        work(2 * stage)
        with jax.named_scope(f"relay{stage}"):
            for k in ((), (0,), (1, 2), (3, 4))[stage - 1]:
                relay(k)
        with jax.named_scope(f"w{stage}"):
            for k in ((), (1, 2), (3, 4), (5, 6))[stage - 1]:
                step_w(k)
        if stage == 1:
            step_a(1)
    perm = jnp.where(interleave, 1.0, 0.0).astype(BF16)
    for n in range(0, D, 512):
        nbp[:, n : n + 512] = jnp.dot(perm, nb[0:ROWS, n : n + 512], preferred_element_type=F32).astype(BF16)
    for d in FAR_FIRST:
        t_copy(d).start()
    with jax.named_scope("relay58"):
        for k in (5, 6):
            relay(k)
    for k in (0, 1, 2):
        send_w(k)
    with jax.named_scope("a5"):
        step_a(5)
    h_copy.wait_recv()
    before = ht[...].astype(F32)
    nb[ROWS:, :] = normalized(jnp.concatenate([before, before], axis=0))
    take(wb.at[0:5, 0:2, 0:4], by_r.at[0])
    take(wb.at[0:11, 0:3, 0], by_r.at[1])

    def w_b(w, first=0, count=NZ):
        return wb[first : first + count, :, w].reshape(count * 128, CH)

    def project(w, rows=ROWS):
        return jnp.dot(nb[0:rows, :], w, preferred_element_type=F32).astype(BF16)

    state_in = jnp.dot(nbp[...], w_b(0), preferred_element_type=F32).astype(BF16)
    xp_s[...] = state_in.astype(F32)
    drive = jnp.dot(state_in, coup[...], preferred_element_type=F32)
    v_re, v_im = drive[:, :FLAT], drive[:, FLAT:]
    a_re, a_im = prm[2:3, :], prm[3:4, :]
    dr[...] = v_re * a_re - v_im * a_im
    di[...] = v_re * a_im + v_im * a_re

    def advance(j, h):
        rows = pl.ds(pl.multiple_of(j * 8, 8), 8)
        b_re, b_im, d_re, d_im = br[rows, :], bi[rows, :], dr[rows, :], di[rows, :]
        re, im = h[0] + d_re, h[1] + d_im
        return (b_re * re - b_im * im - d_re, b_re * im + b_im * re - d_im)

    zero = jnp.zeros((8, FLAT), F32)
    end_re, end_im = lax.fori_loop(0, 32, advance, (zero, zero))
    ec[0] = end_re
    ec[1] = end_im

    def chain(re, im, keep):
        for c in range(8):
            if keep:
                hc[0, c : c + 1, :] = re
                hc[1, c : c + 1, :] = im
            p_re, p_im = pc[0, c : c + 1, :], pc[1, c : c + 1, :]
            re, im = (p_re * re - p_im * im + ec[0, c : c + 1, :], p_re * im + p_im * re + ec[1, c : c + 1, :])
        return re, im

    none = jnp.zeros((1, FLAT), F32)
    e_re, e_im = chain(none, none, False)
    for i in range(4):
        ends[z, i : i + 1, :] = e_re[:, i * 128 : (i + 1) * 128]
        ends[z, 4 + i : 5 + i, :] = e_im[:, i * 128 : (i + 1) * 128]

    def e_copy(d):
        return pltpu.make_async_remote_copy(
            ends.at[z], ends.at[z], e_s, e_r,
            device_id=(lax.rem(z + d, NZ), y, t), device_id_type=MESH)

    for d in FAR_FIRST:
        e_copy(d).start()

    for k in (7, 8):
        relay(k)
    for k in (3, 4, 5, 6):
        send_w(k)
    with jax.named_scope("a6"):
        step_a(6)
    for k in (7, 8):
        step_w(k)
        send_w(k)
    with jax.named_scope("vio_wait"):
        take(wb.at[0:11, 0:2, 0:3], by_r.at[2])
    with jax.named_scope("relay_w04"):
        for k in (0, 1, 2, 3, 4):
            relay_w(k)
    with jax.named_scope("a7"):
        step_a(7, last=True)
    value = project(w_b(1), ROWS + 16).astype(F32)
    inner = project(w_b(2), ROWS + 16).astype(F32)
    gated = (inner * value).astype(BF16).astype(F32)
    ext[8 : 8 + ROWS, :] = gated[:ROWS]
    ext[0:8, :] = jnp.where(z == 0, 0.0, gated[ROWS : ROWS + 8])
    with jax.named_scope("relay_w58"):
        for k in (5, 6, 7, 8):
            relay_w(k)
    outer = project(w_b(3)).astype(F32)
    take(ring_t.at[0:15], tz_r)
    powers = [complex_power(ring_t[j], pk[0, 0:4, :], pk[1, 0:4, :]) for j in range(NZ)]
    filtered = taps[0:1, :] * ext[6 : 6 + ROWS, :] + taps[1:2, :] * ext[7 : 7 + ROWS, :] + taps[2:3, :] * ext[8 : 8 + ROWS, :]
    mix[:, CH:] = (outer * filtered).astype(BF16)

    skip_w = jnp.dot(skip[...], ((iota((16, CH), 1) & 15) == iota((16, CH), 0)).astype(F32), precision=HIGHEST, preferred_element_type=F32)
    skip_l = jnp.sum(jnp.where((iota((8, CH), 1) >> 4) == iota((8, CH), 0), skip_w, 0.0), axis=0, keepdims=True)
    direct = skip_l * xp_s[...]
    way_back[...] = jnp.where(col == (row & 31) * 8 + (row >> 5), 1.0, 0.0).astype(BF16)

    take(ends.at[0:15], e_r)
    re, im = pk[4, 0:4, :], pk[5, 0:4, :]
    in_re, in_im = re, im
    for j in range(NZ):
        p_re, p_im = powers[j]
        re, im = (p_re * re - p_im * im + ends[j, 0:4, :], p_re * im + p_im * re + ends[j, 4:8, :])
        if j < NZ - 1:
            here = z == j + 1
            in_re, in_im = jnp.where(here, re, in_re), jnp.where(here, im, in_im)
    rows8[0, 0:4, :] = in_re
    rows8[0, 4:8, :] = in_im
    rows8[1, 0:4, :] = re
    rows8[1, 4:8, :] = im

    def as_line(n, at):
        return jnp.concatenate([rows8[n, at + i : at + i + 1, :] for i in range(4)], axis=1)

    chain(as_line(0, 0), as_line(0, 4), True)

    def advance2(i, h):
        one = advance(2 * i, h)
        two = advance(2 * i + 1, one)
        rows = pl.ds(pl.multiple_of(i * 16, 16), 16)
        hd[rows, :FLAT] = jnp.concatenate([one[0], two[0]], axis=0).astype(BF16)
        hd[rows, FLAT:] = jnp.concatenate([one[1], two[1]], axis=0).astype(BF16)
        return two

    lax.fori_loop(0, 16, advance2, (hc[0], hc[1]))
    v = lax.dot_general(hd[...], readw[...], NT, preferred_element_type=F32) + direct
    smix = (0.5 * v * (1.0 + jnp.tanh(0.7978845608028654 * (v + 0.044715 * (v * v * v))))).astype(BF16)
    mix[:, :CH] = jnp.dot(way_back[...], smix, preferred_element_type=F32).astype(BF16)

    def rows_of(core):
        return jnp.concatenate([mix[pl.ds(pl.multiple_of(b * 64 + core * 32, 32), 32), :] for b in range(NX)], axis=0)

    def w_out(n):
        return jnp.concatenate([w_b(4, n * NZ // NCHUNK, 2 * NZ // NCHUNK), wa[n * CW : (n + 2) * CW, :]], axis=1)

    def p_copy(n):
        return pltpu.make_async_remote_copy(
            ps.at[n], pr.at[n], p_s, p_r.at[n], device_id=(z, y, xx * 2 + other), device_id_type=MESH)

    def x_copy(n, kind):
        up = 1 if n % 2 == 0 else NX - 1
        d = up if kind < 2 else NX - up
        src = (cs.at[n, lax.rem(xx + 2, NX)], rl.at[n, 1], cs.at[n, lax.rem(xx + NX - up, NX)])[kind]
        dst = (rl.at[n, 0], rb.at[n, 0], rb.at[n, 1])[kind]
        return pltpu.make_async_remote_copy(
            src, dst, x_s, x_r.at[min(kind, 1), n],
            device_id=(z, y, lax.rem(xx + d, NX) * 2 + cc), device_id_type=MESH)

    with jax.named_scope("w_wait"):
        take(wb.at[:, 0:2, 0], by_r.at[3])
    with jax.named_scope("a8"):
        for s in (0, 1):
            a_z(7, s, s).wait_recv()
    theirs, ours = rows_of(other), rows_of(cc)
    for m in range(0, NCHUNK, 2):
        both = lax.dot_general(theirs, w_out(m), NT, preferred_element_type=F32).astype(BF16)
        for n in (m, m + 1):
            ps[n] = both[:, (n - m) * CW : (n - m + 1) * CW]
            p_copy(n).start()
    for m in range(0, NCHUNK, 2):
        both = lax.dot_general(ours, w_out(m), NT, preferred_element_type=F32)
        for n in (m, m + 1):
            p_copy(n).wait_recv()
            part = both[:, (n - m) * CW : (n - m + 1) * CW]
            cs[n] = (part + pr[n].astype(F32)).astype(BF16).reshape(NX, 32, CW)
            x_copy(n, 0).start()
    for n in range(NCHUNK):
        x_copy(n, 2).start()
    far = jnp.where(own, jnp.broadcast_to(as_line(1, 0), (8, FLAT)), 0.0)
    far_i = jnp.where(own, jnp.broadcast_to(as_line(1, 4), (8, FLAT)), 0.0)
    pick = ((iota((4, FLAT), 1) & 63) == z * 4 + iota((4, FLAT), 0)).astype(F32)
    fin[0] = lax.dot_general(pick, far, NT, precision=HIGHEST, preferred_element_type=F32)
    fin[1] = lax.dot_general(pick, far_i, NT, precision=HIGHEST, preferred_element_type=F32)
    for n in range(NCHUNK):
        to = lax.rem(xx + (1 if n % 2 == 0 else NX - 1), NX)
        x_copy(n, 0).wait_recv()
        rl[n, 1] = (rl[n, 0].astype(F32) + cs[n, to].astype(F32)).astype(BF16)
        x_copy(n, 1).start()
    for n in range(NCHUNK):
        take(rb.at[n], x_r.at[1, n])
        total = cs[n, xx].astype(F32) + rb[n, 0].astype(F32) + rb[n, 1].astype(F32)
        out[:, n * CW : (n + 1) * CW] = total.astype(BF16)

    take(wb.at[0, 0, 0:3], ya_s)
    take(wa.at[0:1920, :], az_s)
    take(wb.at[0:12], by_s)
    take(wb.at[0:15, 0], bz_s)
    h_copy.wait_send()
    take(ring_t.at[0:15], tz_s)
    take(ends.at[0:15], e_s)
    take(ps, p_s)
    take(cs.at[0:3], x_s)


def body(
    tokens, norm_gain, w_state_in, w_value, w_outer, w_inner, w_state_out, w_conv_out, log_step, decay_real, frequency,
    step_rate, input_real, input_imag, read_real, read_imag, skip_gain, conv_taps, initial_state,
):
    small = (
        norm_gain.reshape(1, D), log_step.reshape(1, 8), decay_real, frequency, step_rate,
        input_real.transpose(0, 2, 1).reshape(CH, 64), input_imag.transpose(0, 2, 1).reshape(CH, 64), read_real.reshape(CH, 64), read_imag.reshape(CH, 64), skip_gain, conv_taps,
        initial_state.reshape(16, 64),
    )
    dma = pltpu.SemaphoreType.DMA
    anywhere = pl.BlockSpec(memory_space=pl.ANY)
    vmem = pl.BlockSpec(memory_space=pltpu.VMEM)
    mixed, final = pl.pallas_call(
        layer_kernel,
        name="layer",
        out_shape=(pltpu.VMEM((32, D), BF16), pltpu.VMEM((2, 4, 8), F32)),
        in_specs=[anywhere] * (7 + len(small)),
        out_specs=(vmem, vmem),
        scratch_shapes=[pltpu.VMEM(a.shape, a.dtype) for a in small]
        + [
            pltpu.VMEM((D, CH), BF16),
            pltpu.VMEM((NZ, NY, 5, 32, CH), BF16),
            pltpu.VMEM((ROWS, D), BF16),
            pltpu.VMEM((ROWS + 16, D), BF16),
            pltpu.VMEM((ROWS, D), BF16),
            pltpu.VMEM((8, FLAT), F32),
            pltpu.VMEM((6, 8, 128), F32),
            pltpu.VMEM((ROWS, 128), F32),
            pltpu.VMEM((8, 128), F32),
            pltpu.VMEM((NZ, 1, 128), F32),
            pltpu.VMEM((ROWS, FLAT), F32),
            pltpu.VMEM((ROWS, FLAT), F32),
            pltpu.VMEM((2, 8, FLAT), F32),
            pltpu.VMEM((ROWS, FLAT), F32),
            pltpu.VMEM((ROWS, FLAT), F32),
            pltpu.VMEM((CH, 2 * FLAT), BF16),
            pltpu.VMEM((CH, 2 * FLAT), BF16),
            pltpu.VMEM((ROWS, CH), F32),
            pltpu.VMEM((8 + ROWS, CH), F32),
            pltpu.VMEM((8, D), BF16),
            pltpu.VMEM((NZ, 8, 128), F32),
            pltpu.VMEM((2, 8, FLAT), F32),
            pltpu.VMEM((2, 8, FLAT), F32),
            pltpu.VMEM((2, 8, 128), F32),
            pltpu.VMEM((ROWS, 2 * FLAT), BF16),
            pltpu.VMEM((ROWS, ROWS), BF16),
            pltpu.VMEM((ROWS, 2 * CH), BF16),
            pltpu.VMEM((NCHUNK, 128, CW), BF16),
            pltpu.VMEM((NCHUNK, 128, CW), BF16),
            pltpu.VMEM((NCHUNK, NX, 32, CW), BF16),
            pltpu.VMEM((NCHUNK, 2, 32, CW), BF16),
            pltpu.VMEM((NCHUNK, 2, 32, CW), BF16),
            dma((len(small),)),
            dma,
            dma,
            dma, dma,
            dma, dma((2, 8)),
            dma, dma((3, 2, 8)),
            dma, dma((4,)), dma((NZ,)), dma((NZ,)),
            dma, dma,
            dma, dma,
            dma, dma,
            dma, dma((NCHUNK,)),
            dma, dma((2, NCHUNK)),
        ],
        compiler_params=pltpu.CompilerParams(collective_id=0, has_side_effects=True),
    )(tokens.reshape(ROWS, D), w_state_in, w_value, w_inner, w_outer, w_state_out, w_conv_out, *small)
    return (mixed.reshape(1, 32, D), final.transpose(0, 2, 1).reshape(1, 2, 8, 4))


def solution(mesh):
    return jax.shard_map(
        body,
        mesh=mesh,
        in_specs=(
            P("fs", "sp", None),
            P(),
            P(("sp", "fs"), "tp"),
            P(("sp", "fs"), "tp"),
            P(("sp", "fs"), "tp"),
            P(("sp", "fs"), "tp"),
            P(("sp", "fs"), "tp"),
            P(("sp", "fs"), "tp"),
            P("tp"),
            P("tp", None),
            P("tp", None),
            P("fs", "sp"),
            P("tp", None, None),
            P("tp", None, None),
            P("tp", None, None),
            P("tp", None, None),
            P("tp", None),
            P(None, "tp"),
            P("fs", None, "tp", None),
        ),
        out_specs=(P("fs", ("sp", "tp"), None), P("fs", None, "tp", "sp")),
        check_vma=False,
    )
```

```python
import math

import jax
import jax.numpy as jnp
from jax import lax
from jax.experimental import pallas as pl
from jax.experimental.pallas import tpu as pltpu
from jax.sharding import PartitionSpec as P

MESH = pl.DeviceIdType.MESH
HIGHEST = lax.Precision.HIGHEST
F32, BF16 = jnp.float32, jnp.bfloat16
NZ, NY, NX = 16, 4, 4
ROWS, D, CH, FLAT = 256, 2048, 128, 512
NT = (((1,), (1,)), ((), ()))
NCHUNK = 4
CW = D // NCHUNK
NEAR = 3
FAR_FIRST = (8, 7, 9, 6, 10, 5, 11, 4, 12, 3, 13, 2, 14, 1, 15)
SIN = [math.pi, -(math.pi**3) / 6, math.pi**5 / 120, -(math.pi**7) / 5040, math.pi**9 / 362880, -(math.pi**11) / 39916800]
COS = [1.0, -(math.pi**2) / 2, math.pi**4 / 24, -(math.pi**6) / 720, math.pi**8 / 40320, -(math.pi**10) / 3628800, math.pi**12 / 479001600]


def horner(coefs, x):
    total = jnp.full_like(x, coefs[-1])
    for c in coefs[-2::-1]:
        total = total * x + c
    return total


def complex_power(rate, turn, fall):
    u = rate * turn
    r = u - jnp.round(u)
    x = r * r
    s = r * horner(SIN, x)
    c = horner(COS, x)
    grow = jnp.exp2(rate * fall)
    return grow * (1.0 - 2.0 * (s * s)), grow * (2.0 * (s * c))


def iota(shape, dim):
    return lax.broadcasted_iota(jnp.int32, shape, dim)


def lanes4(x):
    return jnp.concatenate([x, x, x, x], axis=1)


def layer_kernel(*refs):
    n_small = 12
    tokens = refs[0]
    shards = refs[1:7]
    small = refs[7 : 7 + n_small]
    out, fin = refs[7 + n_small : 9 + n_small]
    rest = refs[9 + n_small :]
    small_v = rest[:n_small]
    (
        wa, wb, tk, nb, nbp, prm, pk, ratep, tchunk, ring_t, br, bi, pc, dr, di, coup, readw, xp_s, ext, ht,
        ends, ec, hc, rows8, pw, hd, way_back, mix, ps, pr, cs, rl, rb,
        ssem, lsem, tsem, ya_s, ya_r, az_s, az_r, bz_s, bz_r, by_s, by_r, br_r, bw_r, tz_s, tz_r, h_s, h_r, e_s, e_r,
        p_s, p_r, x_s, x_r,
    ) = rest[n_small:]
    gain, lstep, decay, freq, rate, in_r, in_i, rd_r, rd_i, skip, taps, init = small_v
    z = lax.axis_index("sp")
    y = lax.axis_index("fs")
    t = lax.axis_index("tp")
    xx, cc = t // 2, lax.rem(t, 2)
    other = 1 - cc
    zn = lax.rem(z + 1, NZ)

    barrier = pltpu.get_barrier_semaphore()
    for n in (z + 1, z + NZ - 1, z + 2, z + NZ - 2):
        pl.semaphore_signal(barrier, inc=1, device_id=(lax.rem(n, NZ), y, t), device_id_type=MESH)
    for d in range(1, NY):
        pl.semaphore_signal(barrier, inc=1, device_id=(z, lax.rem(y + d, NY), t), device_id_type=MESH)
    for d in (1, NX - 1):
        pl.semaphore_signal(barrier, inc=1, device_id=(z, y, lax.rem(xx + d, NX) * 2 + cc), device_id_type=MESH)
    pl.semaphore_signal(barrier, inc=1, device_id=(z, y, xx * 2 + other), device_id_type=MESH)

    loads = [pltpu.make_async_copy(s, v, ssem.at[n]) for n, (s, v) in enumerate(zip(small, small_v))]
    def take(ref, sem):
        pltpu.make_async_copy(ref, ref, sem).wait()

    local = [pltpu.make_async_copy(shards[w], wb.at[z, y, w], lsem) for w in range(5)]
    mine = pl.ds(pl.multiple_of(z * 128 + y * 32, 32), 32)
    local.append(pltpu.make_async_copy(shards[5], wa.at[mine, :], lsem))
    tok = pltpu.make_async_copy(tokens, tk, tsem)
    for c in local:
        c.start()
    for c in loads:
        c.start()
    tok.start()
    pl.semaphore_wait(barrier, 10)
    take(wb.at[0, 0:2, 0:3], lsem)

    def sides_of(k):
        return (0, 1) if 0 < k < 8 else (0,)

    def at_distance(k, side):
        return lax.rem(z + (k if side else NZ - k), NZ)

    def a_y(d):
        return pltpu.make_async_remote_copy(
            wa.at[mine, :], wa.at[mine, :], ya_s, ya_r, device_id=(z, lax.rem(y + d, NY), t), device_id_type=MESH)

    def a_z(k, side, part=None):
        at = at_distance(k, side) * 128
        rows = pl.ds(pl.multiple_of(at, 128), 128)
        if part is not None:
            rows = pl.ds(pl.multiple_of(at + part * 64, 64), 64)
        return pltpu.make_async_remote_copy(
            wa.at[rows, :], wa.at[rows, :], az_s, az_r.at[side, k],
            device_id=(at_distance(1, 1 - side), y, t), device_id_type=MESH)

    def a_far(side):
        rows = pl.ds(pl.multiple_of(at_distance(6, side) * 128 + side * 64, 64), 64)
        return pltpu.make_async_remote_copy(
            wa.at[rows, :], wa.at[rows, :], az_s, az_r.at[side, 7],
            device_id=(at_distance(2, 1 - side), y, t), device_id_type=MESH)

    def step_a(k):
        for s in (0, 1):
            a_z(k - 1, s).wait_recv()
            if k < 7:
                a_z(k, s).start()
            if k == 6:
                a_far(s).start()

    def of_part(rows, part):
        return rows.at[0] if part == 0 else rows.at[pl.ds(1, 3)] if part == 1 else rows.at[pl.ds(4, 1)]

    def b_z(part, k, side, hop):
        rows = of_part(wb.at[at_distance(k, side), y], part)
        return pltpu.make_async_remote_copy(
            rows, rows, bz_s, bz_r.at[part, side, k + hop - 1],
            device_id=(at_distance(hop, 1 - side), y, t), device_id_type=MESH)

    def w_y(k, side, d, came=0, further=False):
        zb = at_distance(k, side)
        rows = of_part(wb.at[zb, lax.rem(y - came + NY, NY)], 2)
        return pltpu.make_async_remote_copy(
            rows, rows, by_s, bw_r.at[zb] if further else by_r.at[3],
            device_id=(z, lax.rem(y + d, NY), t), device_id_type=MESH)

    def b_y(k, side, d, came=0, further=False):
        zb = at_distance(k, side)
        rows = wb.at[zb, lax.rem(y - came + NY, NY)]
        rows = rows.at[pl.ds(0, 4)] if k < NEAR else of_part(rows, 1)
        return pltpu.make_async_remote_copy(
            rows, rows, by_s, br_r.at[zb] if further else by_r.at[0 if k < NEAR else 2],
            device_id=(z, lax.rem(y + d, NY), t), device_id_type=MESH)

    def s_y(k, side, d):
        rows = wb.at[at_distance(k, side), y, 0]
        return pltpu.make_async_remote_copy(
            rows, rows, by_s, by_r.at[1], device_id=(z, lax.rem(y + d, NY), t), device_id_type=MESH)

    def t_copy(d):
        return pltpu.make_async_remote_copy(
            ring_t.at[z], ring_t.at[z], tz_s, tz_r, device_id=(lax.rem(z + d, NZ), y, t), device_id_type=MESH)

    for part in (0, 1, 2):
        for hop in (2, 1):
            for side in (0, 1):
                b_z(part, 0, side, hop).start()
    for d in (2, 1, 3):
        a_y(d).start()
    b_y(0, 0, 1, further=True).start()
    b_y(0, 0, 3).start()

    for c in loads:
        c.wait()
    row, col = iota((ROWS, ROWS), 0), iota((ROWS, ROWS), 1)
    interleave = col == (row & 7) * 32 + (row >> 3)
    spread = jnp.where(interleave, rate[...], 0.0)
    ratep[...] = jnp.dot(spread, jnp.ones((ROWS, 128), F32), precision=HIGHEST, preferred_element_type=F32)
    totals = jnp.sum(ratep[...].reshape(32, 8, 128), axis=0)
    tchunk[...] = totals
    ring_t[z] = jnp.sum(totals, axis=0, keepdims=True)

    take(wb.at[0, 0, 0:3], ya_r)
    for side in (0, 1):
        a_z(0, side).start()
    h_copy = pltpu.make_async_remote_copy(
        tokens.at[pl.ds(ROWS - 8, 8), :], ht, h_s, h_r, device_id=(zn, y, t), device_id_type=MESH)
    h_copy.start()

    tall = jnp.concatenate([decay[...], freq[...], init[...]], axis=0)
    hot = ((iota((64, FLAT), 1) & 63) == iota((64, FLAT), 0)).astype(F32)
    wide = jnp.dot(tall, hot, precision=HIGHEST, preferred_element_type=F32)
    own = (iota((8, FLAT), 1) >> 6) == iota((8, FLAT), 0)

    def line(v):
        return jnp.sum(jnp.where(own, v, 0.0), axis=0, keepdims=True)

    decay_l, freq_l = line(wide[0:8]), line(wide[8:16])
    column = jnp.sum(jnp.where(iota((8, 8), 0) == iota((8, 8), 1), lstep[...], 0.0), axis=1, keepdims=True)
    dt = jnp.exp(line(jnp.broadcast_to(column, (8, FLAT))))
    modulus = decay_l * decay_l + freq_l * freq_l
    lines = [dt * freq_l * (0.5 / math.pi), dt * decay_l * math.log2(math.e), decay_l / modulus, -freq_l / modulus,
             line(wide[16:24]), line(wide[24:32])]
    for n, v in enumerate(lines):
        prm[n : n + 1, :] = v
        for i in range(4):
            pk[n, i : i + 1, :] = v[:, i * 128 : (i + 1) * 128]
    c_re, c_im = complex_power(lanes4(tchunk[...]), prm[0:1, :], prm[1:2, :])
    pc[0] = c_re
    pc[1] = c_im
    block_t = (iota((CH, FLAT), 1) >> 6) == (iota((CH, FLAT), 0) >> 4)
    hot64 = hot.astype(BF16)
    for n, (dst, src, sign) in enumerate(((coup, in_r, 1), (coup, in_i, 1), (readw, rd_r, 1), (readw, rd_i, -1))):
        w = jnp.dot(src[...].astype(BF16), hot64, preferred_element_type=F32)
        at = (n % 2) * FLAT
        dst[:, at : at + FLAT] = jnp.where(block_t, sign * w, 0.0).astype(BF16)
    tok.wait()

    def normalized(f):
        mean_square = jnp.mean(f * f, axis=-1, keepdims=True)
        return (f * lax.rsqrt(mean_square + 1e-06) * gain[...]).astype(BF16)

    def work(k):
        rows = pl.ds(pl.multiple_of((k - 1) * 32, 32), 32)
        nb[rows, :] = normalized(tk[rows, :].astype(F32))
        for half in range(2):
            rows = pl.ds(pl.multiple_of((k - 1) * 32 + half * 16, 16), 16)
            re, im = complex_power(lanes4(ratep[rows, :]), prm[0:1, :], prm[1:2, :])
            br[rows, :] = re
            bi[rows, :] = im

    def step_w(k):
        for s in sides_of(k):
            b_z(2, k - 1, s, 1).wait_recv()
            if k + 2 <= (7 if s else 8):
                b_z(2, k, s, 2).start()

    def send_w(k):
        for s in sides_of(k):
            for d in (1, 3) if k < 5 else (2, 1, 3):
                w_y(k, s, d, further=k < 5 and d == (3 if s else 1)).start()

    def relay_w(k):
        for s in (0, 1) if 0 < k < 8 else (0,):
            d = 3 if s else 1
            w_y(k, s, d, further=True).wait_recv()
            w_y(k, s, d, d).start()

    def step_b(pair, between):
        for part in (0, 1):
            for k in pair:
                for s in sides_of(k):
                    b_z(part, k - 1, s, 1).wait_recv()
                    if k + 2 <= (7 if s else 8):
                        b_z(part, k, s, 2).start()
                    if k >= NEAR and part == 0:
                        for d in (2, 1, 3):
                            s_y(k, s, d).start()
            if part == 0 and between:
                step_a(between)
        for k in pair:
            for s in sides_of(k):
                for d in (1, 3):
                    b_y(k, s, d, further=d == (3 if s else 1)).start()

    def relay(k):
        for s in (0, 1) if 0 < k < 8 else (0,):
            d = 3 if s else 1
            b_y(k, s, d, further=True).wait_recv()
            b_y(k, s, d, d).start()

    for stage in range(1, 5):
        with jax.named_scope(f"b{stage}"):
            step_b((2 * stage - 1, 2 * stage), stage if stage > 1 else None)
        work(2 * stage - 1)
        work(2 * stage)
        with jax.named_scope(f"relay{stage}"):
            for k in ((), (0,), (1, 2), (3, 4))[stage - 1]:
                relay(k)
        with jax.named_scope(f"w{stage}"):
            for k in ((), (1, 2), (3, 4), (5, 6))[stage - 1]:
                step_w(k)
        if stage == 1:
            step_a(1)
    perm = jnp.where(interleave, 1.0, 0.0).astype(BF16)
    for n in range(0, D, 512):
        nbp[:, n : n + 512] = jnp.dot(perm, nb[0:ROWS, n : n + 512], preferred_element_type=F32).astype(BF16)
    for d in FAR_FIRST:
        t_copy(d).start()
    with jax.named_scope("relay58"):
        for k in (5, 6):
            relay(k)
    for k in (0, 1, 2):
        send_w(k)
    with jax.named_scope("a5"):
        step_a(5)
    h_copy.wait_recv()
    before = ht[...].astype(F32)
    nb[ROWS:, :] = normalized(jnp.concatenate([before, before], axis=0))
    take(wb.at[0:5, 0:2, 0:4], by_r.at[0])
    take(wb.at[0:11, 0:3, 0], by_r.at[1])

    def w_b(w, first=0, count=NZ):
        return wb[first : first + count, :, w].reshape(count * 128, CH)

    def project(w, rows=ROWS):
        return jnp.dot(nb[0:rows, :], w, preferred_element_type=F32).astype(BF16)

    state_in = jnp.dot(nbp[...], w_b(0), preferred_element_type=F32).astype(BF16)
    xp_s[...] = state_in.astype(F32)
    drive = jnp.dot(state_in, coup[...], preferred_element_type=F32)
    v_re, v_im = drive[:, :FLAT], drive[:, FLAT:]
    a_re, a_im = prm[2:3, :], prm[3:4, :]
    dr[...] = v_re * a_re - v_im * a_im
    di[...] = v_re * a_im + v_im * a_re

    def advance(j, h):
        rows = pl.ds(pl.multiple_of(j * 8, 8), 8)
        b_re, b_im, d_re, d_im = br[rows, :], bi[rows, :], dr[rows, :], di[rows, :]
        re, im = h[0] + d_re, h[1] + d_im
        return (b_re * re - b_im * im - d_re, b_re * im + b_im * re - d_im)

    zero = jnp.zeros((8, FLAT), F32)
    end_re, end_im = lax.fori_loop(0, 32, advance, (zero, zero))
    ec[0] = end_re
    ec[1] = end_im

    def chain(re, im, keep):
        for c in range(8):
            if keep:
                hc[0, c : c + 1, :] = re
                hc[1, c : c + 1, :] = im
            p_re, p_im = pc[0, c : c + 1, :], pc[1, c : c + 1, :]
            re, im = (p_re * re - p_im * im + ec[0, c : c + 1, :], p_re * im + p_im * re + ec[1, c : c + 1, :])
        return re, im

    none = jnp.zeros((1, FLAT), F32)
    e_re, e_im = chain(none, none, False)
    for i in range(4):
        ends[z, i : i + 1, :] = e_re[:, i * 128 : (i + 1) * 128]
        ends[z, 4 + i : 5 + i, :] = e_im[:, i * 128 : (i + 1) * 128]

    def e_copy(d):
        return pltpu.make_async_remote_copy(
            ends.at[z], ends.at[z], e_s, e_r.at[z],
            device_id=(lax.rem(z + d, NZ), y, t), device_id_type=MESH)

    for d in FAR_FIRST:
        e_copy(d).start()

    for k in (7, 8):
        relay(k)
    for k in (3, 4, 5, 6):
        send_w(k)
    with jax.named_scope("a6"):
        step_a(6)
    for k in (7, 8):
        step_w(k)
        send_w(k)
    with jax.named_scope("relay_w02"):
        for k in (0, 1, 2):
            relay_w(k)
    with jax.named_scope("vio_wait"):
        take(wb.at[0:11, 0:2, 0:3], by_r.at[2])
    with jax.named_scope("relay_w04"):
        for k in (3, 4):
            relay_w(k)
    value = project(w_b(1), ROWS + 16).astype(F32)
    inner = project(w_b(2), ROWS + 16).astype(F32)
    gated = (inner * value).astype(BF16).astype(F32)
    ext[8 : 8 + ROWS, :] = gated[:ROWS]
    ext[0:8, :] = jnp.where(z == 0, 0.0, gated[ROWS : ROWS + 8])
    outer = project(w_b(3)).astype(F32)
    take(ring_t.at[0:15], tz_r)
    for j in range(NZ):
        pw[j, 0], pw[j, 1] = complex_power(ring_t[j], pk[0, 0:4, :], pk[1, 0:4, :])
    filtered = taps[0:1, :] * ext[6 : 6 + ROWS, :] + taps[1:2, :] * ext[7 : 7 + ROWS, :] + taps[2:3, :] * ext[8 : 8 + ROWS, :]
    mix[:, CH:] = (outer * filtered).astype(BF16)

    skip_w = jnp.dot(skip[...], ((iota((16, CH), 1) & 15) == iota((16, CH), 0)).astype(F32), precision=HIGHEST, preferred_element_type=F32)
    skip_l = jnp.sum(jnp.where((iota((8, CH), 1) >> 4) == iota((8, CH), 0), skip_w, 0.0), axis=0, keepdims=True)
    direct = skip_l * xp_s[...]
    way_back[...] = jnp.where(col == (row & 31) * 8 + (row >> 5), 1.0, 0.0).astype(BF16)

    def through(j, h):
        return (pw[j, 0] * h[0] - pw[j, 1] * h[1] + ends[j, 0:4, :], pw[j, 0] * h[1] + pw[j, 1] * h[0] + ends[j, 4:8, :])

    def next_span(j, h):
        take(ends.at[j], e_r.at[j])
        return through(j, h)

    in_re, in_im = lax.fori_loop(0, z, next_span, (pk[4, 0:4, :], pk[5, 0:4, :]))
    rows8[0, 0:4, :] = in_re
    rows8[0, 4:8, :] = in_im

    def as_line(n, at):
        return jnp.concatenate([rows8[n, at + i : at + i + 1, :] for i in range(4)], axis=1)

    chain(as_line(0, 0), as_line(0, 4), True)

    def advance2(i, h):
        one = advance(2 * i, h)
        two = advance(2 * i + 1, one)
        rows = pl.ds(pl.multiple_of(i * 16, 16), 16)
        hd[rows, :FLAT] = jnp.concatenate([one[0], two[0]], axis=0).astype(BF16)
        hd[rows, FLAT:] = jnp.concatenate([one[1], two[1]], axis=0).astype(BF16)
        return two

    lax.fori_loop(0, 16, advance2, (hc[0], hc[1]))
    v = lax.dot_general(hd[...], readw[...], NT, preferred_element_type=F32) + direct
    smix = (0.5 * v * (1.0 + jnp.tanh(0.7978845608028654 * (v + 0.044715 * (v * v * v))))).astype(BF16)
    mix[:, :CH] = jnp.dot(way_back[...], smix, preferred_element_type=F32).astype(BF16)

    def rows_of(core):
        return jnp.concatenate([mix[pl.ds(pl.multiple_of(b * 64 + core * 32, 32), 32), :] for b in range(NX)], axis=0)

    def w_out(n):
        return jnp.concatenate([w_b(4, n * NZ // NCHUNK, 2 * NZ // NCHUNK), wa[n * CW : (n + 2) * CW, :]], axis=1)

    def p_copy(n):
        return pltpu.make_async_remote_copy(
            ps.at[n], pr.at[n], p_s, p_r.at[n], device_id=(z, y, xx * 2 + other), device_id_type=MESH)

    def x_copy(n, kind):
        up = 1 if n % 2 == 0 else NX - 1
        d = up if kind < 2 else NX - up
        src = (cs.at[n, lax.rem(xx + 2, NX)], rl.at[n, 1], cs.at[n, lax.rem(xx + NX - up, NX)])[kind]
        dst = (rl.at[n, 0], rb.at[n, 0], rb.at[n, 1])[kind]
        return pltpu.make_async_remote_copy(
            src, dst, x_s, x_r.at[min(kind, 1), n],
            device_id=(z, y, lax.rem(xx + d, NX) * 2 + cc), device_id_type=MESH)

    with jax.named_scope("w_wait"):
        take(wb.at[0:13, 0:3, 0], by_r.at[3])
    with jax.named_scope("a8"):
        step_a(7)
        for s in (0, 1):
            a_z(7, s, s).wait_recv()
    theirs, ours = rows_of(other), rows_of(cc)
    for m in range(0, NCHUNK, 2):
        both = lax.dot_general(theirs, w_out(m), NT, preferred_element_type=F32).astype(BF16)
        for n in (m, m + 1):
            ps[n] = both[:, (n - m) * CW : (n - m + 1) * CW]
            p_copy(n).start()
    for m in range(0, NCHUNK, 2):
        both = lax.dot_general(ours, w_out(m), NT, preferred_element_type=F32)
        for n in (m, m + 1):
            p_copy(n).wait_recv()
            part = both[:, (n - m) * CW : (n - m + 1) * CW]
            cs[n] = (part + pr[n].astype(F32)).astype(BF16).reshape(NX, 32, CW)
            x_copy(n, 0).start()
    for n in range(NCHUNK):
        x_copy(n, 2).start()
    re, im = lax.fori_loop(z + 1, NZ, next_span, through(z, (in_re, in_im)))
    rows8[1, 0:4, :] = re
    rows8[1, 4:8, :] = im
    far = jnp.where(own, jnp.broadcast_to(as_line(1, 0), (8, FLAT)), 0.0)
    far_i = jnp.where(own, jnp.broadcast_to(as_line(1, 4), (8, FLAT)), 0.0)
    pick = ((iota((4, FLAT), 1) & 63) == z * 4 + iota((4, FLAT), 0)).astype(F32)
    fin[0] = lax.dot_general(pick, far, NT, precision=HIGHEST, preferred_element_type=F32)
    fin[1] = lax.dot_general(pick, far_i, NT, precision=HIGHEST, preferred_element_type=F32)
    for n in range(NCHUNK):
        to = lax.rem(xx + (1 if n % 2 == 0 else NX - 1), NX)
        x_copy(n, 0).wait_recv()
        rl[n, 1] = (rl[n, 0].astype(F32) + cs[n, to].astype(F32)).astype(BF16)
        x_copy(n, 1).start()
    for n in range(NCHUNK):
        take(rb.at[n], x_r.at[1, n])
        total = cs[n, xx].astype(F32) + rb[n, 0].astype(F32) + rb[n, 1].astype(F32)
        out[:, n * CW : (n + 1) * CW] = total.astype(BF16)

    take(wb.at[0, 0, 0:3], ya_s)
    take(wa.at[0:1920, :], az_s)
    take(wb.at[0:12], by_s)
    take(wb.at[0:15, 0], bz_s)
    h_copy.wait_send()
    take(ring_t.at[0:15], tz_s)
    take(ends.at[0:15], e_s)
    take(ps, p_s)
    take(cs.at[0:3], x_s)


def body(
    tokens, norm_gain, w_state_in, w_value, w_outer, w_inner, w_state_out, w_conv_out, log_step, decay_real, frequency,
    step_rate, input_real, input_imag, read_real, read_imag, skip_gain, conv_taps, initial_state,
):
    small = (
        norm_gain.reshape(1, D), log_step.reshape(1, 8), decay_real, frequency, step_rate,
        input_real.transpose(0, 2, 1).reshape(CH, 64), input_imag.transpose(0, 2, 1).reshape(CH, 64), read_real.reshape(CH, 64), read_imag.reshape(CH, 64), skip_gain, conv_taps,
        initial_state.reshape(16, 64),
    )
    dma = pltpu.SemaphoreType.DMA
    anywhere = pl.BlockSpec(memory_space=pl.ANY)
    vmem = pl.BlockSpec(memory_space=pltpu.VMEM)
    mixed, final = pl.pallas_call(
        layer_kernel,
        name="layer",
        out_shape=(pltpu.VMEM((32, D), BF16), pltpu.VMEM((2, 4, 8), F32)),
        in_specs=[anywhere] * (7 + len(small)),
        out_specs=(vmem, vmem),
        scratch_shapes=[pltpu.VMEM(a.shape, a.dtype) for a in small]
        + [
            pltpu.VMEM((D, CH), BF16),
            pltpu.VMEM((NZ, NY, 5, 32, CH), BF16),
            pltpu.VMEM((ROWS, D), BF16),
            pltpu.VMEM((ROWS + 16, D), BF16),
            pltpu.VMEM((ROWS, D), BF16),
            pltpu.VMEM((8, FLAT), F32),
            pltpu.VMEM((6, 8, 128), F32),
            pltpu.VMEM((ROWS, 128), F32),
            pltpu.VMEM((8, 128), F32),
            pltpu.VMEM((NZ, 1, 128), F32),
            pltpu.VMEM((ROWS, FLAT), F32),
            pltpu.VMEM((ROWS, FLAT), F32),
            pltpu.VMEM((2, 8, FLAT), F32),
            pltpu.VMEM((ROWS, FLAT), F32),
            pltpu.VMEM((ROWS, FLAT), F32),
            pltpu.VMEM((CH, 2 * FLAT), BF16),
            pltpu.VMEM((CH, 2 * FLAT), BF16),
            pltpu.VMEM((ROWS, CH), F32),
            pltpu.VMEM((8 + ROWS, CH), F32),
            pltpu.VMEM((8, D), BF16),
            pltpu.VMEM((NZ, 8, 128), F32),
            pltpu.VMEM((2, 8, FLAT), F32),
            pltpu.VMEM((2, 8, FLAT), F32),
            pltpu.VMEM((2, 8, 128), F32),
            pltpu.VMEM((NZ, 2, 4, 128), F32),
            pltpu.VMEM((ROWS, 2 * FLAT), BF16),
            pltpu.VMEM((ROWS, ROWS), BF16),
            pltpu.VMEM((ROWS, 2 * CH), BF16),
            pltpu.VMEM((NCHUNK, 128, CW), BF16),
            pltpu.VMEM((NCHUNK, 128, CW), BF16),
            pltpu.VMEM((NCHUNK, NX, 32, CW), BF16),
            pltpu.VMEM((NCHUNK, 2, 32, CW), BF16),
            pltpu.VMEM((NCHUNK, 2, 32, CW), BF16),
            dma((len(small),)),
            dma,
            dma,
            dma, dma,
            dma, dma((2, 8)),
            dma, dma((3, 2, 8)),
            dma, dma((4,)), dma((NZ,)), dma((NZ,)),
            dma, dma,
            dma, dma,
            dma, dma((NZ,)),
            dma, dma((NCHUNK,)),
            dma, dma((2, NCHUNK)),
        ],
        compiler_params=pltpu.CompilerParams(collective_id=0, has_side_effects=True),
    )(tokens.reshape(ROWS, D), w_state_in, w_value, w_inner, w_outer, w_state_out, w_conv_out, *small)
    return (mixed.reshape(1, 32, D), final.transpose(0, 2, 1).reshape(1, 2, 8, 4))


def solution(mesh):
    return jax.shard_map(
        body,
        mesh=mesh,
        in_specs=(
            P("fs", "sp", None),
            P(),
            P(("sp", "fs"), "tp"),
            P(("sp", "fs"), "tp"),
            P(("sp", "fs"), "tp"),
            P(("sp", "fs"), "tp"),
            P(("sp", "fs"), "tp"),
            P(("sp", "fs"), "tp"),
            P("tp"),
            P("tp", None),
            P("tp", None),
            P("fs", "sp"),
            P("tp", None, None),
            P("tp", None, None),
            P("tp", None, None),
            P("tp", None, None),
            P("tp", None),
            P(None, "tp"),
            P("fs", None, "tp", None),
        ),
        out_specs=(P("fs", ("sp", "tp"), None), P("fs", None, "tp", "sp")),
        check_vma=False,
    )
```
